32 devices in a mesh: sp: 8 (over z, core), tp: 4 (over y, x).
Axes of the slice: x: 2, y: 2, z: 4, core: 2. Of those that a mesh axis runs over, the one named last changes fastest.
Arguments:
- residual: bfloat16 [2048, 4096], P('sp', 'tp'), may hold values from -6 to 6
- pool_in: bfloat16 [2048, 2048], P('sp', 'tp'), may hold values from -6 to 6
- docs: int32 [2048], P('sp'), may hold values from 0 to 3, never falling along the last dimension, each value on 1 to 1024 neighbouring positions
- pool_weight: bfloat16 [16, 128, 128], P('tp'), may hold values from -0.5 to 0.5
- pool_gain: float32 [2048], P('tp'), may hold values from 0.1 to 1.9
- out_weight: bfloat16 [2048, 4096], P(None, 'tp'), may hold values from -0.125 to 0.125
- norm_gain: float32 [4096], replicated, may hold values from 0.1 to 1.9
- routes: int32 [2048, 2], P('sp'), may hold values from 0 to 7, all different within a row; in each aligned block of 256 rows (0 to 255, 256 to 511, ...) at most 96 rows name the same one
- route_weights: float32 [2048, 2], P('sp'), may hold values from 0.25 to 1
- w_gate: bfloat16 [8, 4096, 2048], P('sp', None, 'tp'), may hold values from -0.09375 to 0.09375
- w_up: bfloat16 [8, 4096, 2048], P('sp', None, 'tp'), may hold values from -0.09375 to 0.09375
- w_down: bfloat16 [8, 2048, 4096], P('sp', None, 'tp'), may hold values from -0.125 to 0.125
Outputs:
- layer_out: bfloat16 [2048, 4096], P('sp', 'tp')
The draws below stay inside these ranges and needn't reach their ends.
Inputs may be any that keep to these rules, and one draw needn't show every extreme that they name: `docs`: document numbers never fall along the sequence; each document has at most 1024 positions. `routes`: each token names 2 different experts; among the tokens of one index of sp (aligned blocks of 256 rows) no expert is named more than 96 times, a bound that some block reaches.
All inputs are finite; a program needn't handle non-finite values.
Results may differ from the reference program's by a relative error of at most 0.012.
Values may be sent and summed in bfloat16 or wider, within the bound.
A program may use at most 64 MiB of HBM per device.

```python
import math
import jax
import jax.numpy as jnp
import numpy as np
from jax import lax

D = 4096
DFF = 2048
GD = 128
POOL_GROUPS = 16
TOPK = 2
TOK_DEV = 256
POOL_WIDTH = 2048
EXPERTS = 8
TOKENS = 2048
CAP = 96
DOCS = 4
DOC_MOST = 1024
N_SP = 8


def steps_of(stream_key, dims, split, least, top_value):
    factor_of, own = 1.0, jax.random.fold_in(stream_key, 6)
    for axis_at, parts in split:
        heights = jnp.exp(jax.random.uniform(jax.random.fold_in(own, axis_at), (parts,), jnp.float32, least / len(split), top_value / len(split)))
        factor_of = factor_of * jnp.repeat(heights, dims[axis_at] // parts).reshape([-1 if axis == axis_at else 1 for axis in range(len(dims))])
    return factor_of


def length_profile(number_of, total, most, slope):
    loads = [(1 << 20) // math.isqrt(rank ** slope) + 1 for rank in range(2, number_of + 1)]
    spare, given = total - most - (number_of - 1), [1] * (number_of - 1)
    while spare > 0:
        movable = [i for i in range(number_of - 1) if given[i] < most]
        whole, remaining = sum([loads[i] for i in movable]), spare
        for i in movable:
            extra = min(most - given[i], max(1, remaining * loads[i] // whole), spare)
            given[i] = given[i] + extra
            spare = spare - extra
    return np.array([most] + given)


def uneven_parts(key, count, total, bound, lean):
    if count == 2:
        one = jax.random.randint(key, (), max(1, total - bound), min(bound, total - 1) + 1)
        return jnp.stack([one, total - one])
    sizes = jnp.asarray(length_profile(count, total, bound, lean), jnp.int32)
    twos = (count - 1) // 2
    giver, sink = sizes[1:1 + 2 * twos:2], sizes[2:2 + 2 * twos:2]
    room = jnp.minimum(giver - 1, bound - sink)
    moved = jax.random.randint(jax.random.fold_in(key, 1), (twos,), 0, 1 << 20) % (room + 1)
    sizes = sizes.at[1:1 + 2 * twos:2].set(giver - moved).at[2:2 + 2 * twos:2].set(sink + moved)
    return sizes[jax.random.permutation(jax.random.fold_in(key, 2), count)]


def routed_block(rng, own, number, rows, amount, top, limit, slope):
    ranking = jax.random.permutation(rng, amount)
    crowded, common = load_shares(amount, rows * top, limit, slope, True), load_shares(amount, rows * top, limit, slope, False)
    places = jnp.arange(amount)

    def named(tallies, turn):
        used = int((tallies > 0).sum())
        fixed = max(1, used // 4)
        moved = fixed + (places - fixed + turn * (used - fixed)) % max(1, amount - fixed)
        return jnp.zeros((amount,), jnp.int32).at[ranking[jnp.where(places < fixed, places, moved)]].set(jnp.asarray(tallies, jnp.int32))

    tallies = jnp.where(number % 4 == 0, named(crowded, number // 4), named(common, number - number // 4 - 1))
    mixed = jax.random.permutation(jax.random.fold_in(own, 3), amount)
    giver, sink = mixed[0:amount // 2 * 2:2], mixed[1:amount // 2 * 2:2]
    slack = jnp.minimum(tallies[giver] - 1, limit - tallies[sink]) // 2
    slack = jnp.where((giver == ranking[0]) | (sink == ranking[0]) | (tallies[sink] == 0), 0, jnp.maximum(slack, 0))
    moved = jax.random.randint(jax.random.fold_in(own, 4), (amount // 2,), 0, 1 << 20) % (slack + 1)
    tallies = tallies.at[giver].add(-moved).at[sink].add(moved)
    items = jnp.searchsorted(jnp.cumsum(tallies), jnp.arange(rows * top), side="right").astype(jnp.int32)
    grid = items.reshape(top, rows).T
    grid = grid[jax.random.permutation(jax.random.fold_in(own, 1), rows)]
    turn = jax.random.randint(jax.random.fold_in(own, 2), (rows, 1), 0, top)
    return jnp.take_along_axis(grid, (jnp.arange(top)[None, :] + turn) % top, axis=1)


def load_shares(number_of, total, reach, slope, full):
    portions = [(1 << 20) // math.isqrt(standing ** slope) + 1 for standing in range(1, number_of + 1)]
    largest = reach if full else min(reach, max(-(-total // number_of), total * portions[0] // sum(portions)))
    least = 1 if total - largest >= number_of - 1 else 0
    holding, spare = [largest] + [least] * (number_of - 1), total - largest - least * (number_of - 1)
    while spare > 0:
        candidates = [i for i in range(1, number_of) if holding[i] < largest] or [i for i in range(1, number_of) if holding[i] < reach]
        whole, budget = sum([portions[i] for i in candidates]), spare
        for i in candidates:
            addition = min(reach - holding[i], max(1, budget * portions[i] // whole), spare)
            holding[i] = holding[i] + addition
            spare = spare - addition
    return np.array(holding)


def bell_draw(own_key, extent, deviation, most, shards=(), held_as=jnp.bfloat16):
    drawn = deviation * jax.random.normal(own_key, extent, jnp.float32)
    if shards:
        drawn = drawn * steps_of(own_key, extent, shards, -0.22, 0.18)
    return jnp.clip(drawn, -most, most).astype(held_as)


def setup_inputs(seed: int = 0) -> dict:
    key_list = jax.random.split(jax.random.key(seed), 13)
    residual = bell_draw(key_list[0], (TOKENS, D), 1.0, 6.0, ((0, 8), (1, 4)))
    pool_in = bell_draw(key_list[1], (TOKENS, POOL_WIDTH), 1.0, 6.0, ((0, 8), (1, 4)))
    docs = jnp.searchsorted(jnp.cumsum(uneven_parts(key_list[2], DOCS, TOKENS, DOC_MOST, 1)), jnp.arange(TOKENS), side="right").astype(jnp.int32)
    pool_weight = bell_draw(key_list[3], (POOL_GROUPS, GD, GD), GD ** -0.5, 0.5, ((0, 4),))
    pool_gain = jnp.clip(1.0 + 0.18 * jax.random.normal(key_list[4], (POOL_WIDTH,), jnp.float32), 0.1, 1.9)
    out_weight = bell_draw(key_list[5], (POOL_WIDTH, D), POOL_WIDTH ** -0.5, 0.125, ((1, 4),))
    norm_gain = jnp.clip(1.0 + 0.18 * jax.random.normal(key_list[6], (D,), jnp.float32), 0.1, 1.9)
    routes_keys = jax.random.split(jax.random.fold_in(key_list[7], 1), TOKENS // TOK_DEV)
    routes_turns = jax.random.permutation(jax.random.fold_in(key_list[7], 3), TOKENS // TOK_DEV)
    routes = jax.vmap(lambda own, number: routed_block(jax.random.fold_in(key_list[7], 2), own, number, TOK_DEV, EXPERTS, TOPK, CAP, 1))(routes_keys, routes_turns).reshape((TOKENS, TOPK))
    route_weights = jnp.clip(0.25 + 0.75 * jax.random.uniform(key_list[8], (TOKENS, TOPK), jnp.float32) ** steps_of(key_list[8], (TOKENS, TOPK), ((0, 8),), -0.2, 0.2), 0.25, 1.0)
    w_gate = bell_draw(key_list[9], (EXPERTS, D, DFF), D ** -0.5, 0.09375, ((0, 8), (2, 4)))
    w_up = bell_draw(key_list[10], (EXPERTS, D, DFF), D ** -0.5, 0.09375, ((0, 8), (2, 4)))
    w_down = bell_draw(key_list[11], (EXPERTS, DFF, D), DFF ** -0.5, 0.125, ((0, 8), (2, 4)))
    return {"residual": residual, "pool_in": pool_in, "docs": docs, "pool_weight": pool_weight, "pool_gain": pool_gain, "out_weight": out_weight, "norm_gain": norm_gain, "routes": routes, "route_weights": route_weights, "w_gate": w_gate, "w_up": w_up, "w_down": w_down}


EPS = 1e-06

def pool_mix(pool_in, docs, pool_weight, pool_gain):
    length = pool_in.shape[0]
    values = pool_in.astype(jnp.float32)
    places = jnp.arange(length)
    group_of = jnp.arange(POOL_WIDTH) // GD
    span = 2 ** (1 + group_of % 4)
    totals = jnp.zeros((length, POOL_WIDTH), jnp.float32)
    counts = jnp.zeros((length, POOL_WIDTH), jnp.float32)
    for offset in range(16):
        shifted = jnp.pad(values, ((offset, 0), (0, 0)))[:length]
        prior = jnp.pad(docs, (offset, 0))[:length]
        same = ((places >= offset) & (prior == docs)).astype(jnp.float32)[:, None]
        inside = (offset < span).astype(jnp.float32)[None, :]
        weight = same * inside
        totals = totals + weight * shifted
        counts = counts + weight
    diff = (totals / counts - values).astype(jnp.bfloat16)
    mixed = jnp.einsum('tgc,gcd->tgd', diff.reshape(length, POOL_GROUPS, GD).astype(jnp.float32), pool_weight.astype(jnp.float32))
    return (mixed.reshape(length, POOL_WIDTH) * pool_gain).astype(jnp.bfloat16)

def expert_apply(packed):
    rows, gate_w, up_w, down_w = packed
    gate = jnp.dot(rows, gate_w, preferred_element_type=jnp.float32)
    up = jnp.dot(rows, up_w, preferred_element_type=jnp.float32)
    act = (jax.nn.silu(gate) * up).astype(jnp.bfloat16)
    return jnp.dot(act, down_w, preferred_element_type=jnp.float32).astype(jnp.bfloat16)

def reference(residual, pool_in, docs, pool_weight, pool_gain, out_weight, norm_gain, routes, route_weights, w_gate, w_up, w_down):
    pooled = pool_mix(pool_in, docs, pool_weight, pool_gain)
    proj = jnp.dot(pooled, out_weight, preferred_element_type=jnp.float32)
    updated = (residual.astype(jnp.float32) + proj).astype(jnp.bfloat16)
    upf = updated.astype(jnp.float32)
    normed = (upf * lax.rsqrt(lax.optimization_barrier(jnp.mean(upf * upf, axis=1, keepdims=True)) + EPS) * norm_gain).astype(jnp.bfloat16)
    ids = routes.reshape(N_SP, TOK_DEV * TOPK)
    onehot = (ids[:, :, None] == jnp.arange(EXPERTS)[None, None, :]).astype(jnp.int32)
    rank = lax.optimization_barrier(jnp.sum(onehot * (jnp.cumsum(onehot, axis=1) - 1), axis=2))
    blocks = jnp.arange(N_SP)[:, None]
    flat = (ids * (N_SP * CAP) + blocks * CAP + rank).reshape(-1).astype(jnp.int32)
    source = (blocks * TOK_DEV + jnp.arange(TOK_DEV * TOPK)[None, :] // TOPK).reshape(-1).astype(jnp.int32)
    buffer = jnp.zeros((EXPERTS * N_SP * CAP, D), jnp.bfloat16).at[flat].set(normed[source])
    results = lax.map(expert_apply, (buffer.reshape(EXPERTS, N_SP * CAP, D), w_gate, w_up, w_down))
    picked = results.reshape(EXPERTS * N_SP * CAP, D)[flat].reshape(TOKENS, TOPK, D)
    combined = upf + lax.optimization_barrier(jnp.sum(route_weights[:, :, None] * picked.astype(jnp.float32), axis=1))
    return combined.astype(jnp.bfloat16)
```

```python
import functools

import jax
import jax.numpy as jnp
from jax import lax
from jax.experimental import pallas as pl
from jax.experimental.pallas import tpu as pltpu
from jax.sharding import PartitionSpec as P

GD = 128
TOPK = 2
EPS = 1e-06
MESH = pl.DeviceIdType.MESH
CORES = 2
LANES = 128
TAIL = 16
VMEM_LIMIT = 62 * 1024 * 1024


def remote(src, dst, send_sem, recv_sem, device):
    return pltpu.make_async_remote_copy(
        src_ref=src,
        dst_ref=dst,
        send_sem=send_sem,
        recv_sem=recv_sem,
        device_id=device,
        device_id_type=MESH,
    )


class Spread:
    def __init__(self, n_tp, sp, tp, block, send_sem, recv_sem):
        self.n_tp, self.sp, self.tp = n_tp, sp, tp
        self.block, self.send_sem, self.recv_sem = block, send_sem, recv_sem
        self.relay = n_tp == 4
        self.across = 2 * (tp // 2) + 1 - tp % 2
        self.along = (tp + 2) % 4

    def copy(self, owner, piece, sem, peer):
        ref = self.block(owner, piece)
        return remote(ref, ref, self.send_sem(sem), self.recv_sem(owner, piece), (self.sp, peer))

    def direct(self):
        if self.relay:
            return [
                self.copy(self.tp, 0, 0, self.across),
                self.copy(self.tp, 1, 1, self.along),
                self.copy(self.tp, 1, 2, self.across),
                self.copy(self.tp, 0, 3, self.along),
            ]
        return [
            self.copy(self.tp, 0, j - 1, lax.rem(self.tp + j, self.n_tp)) for j in range(1, self.n_tp)
        ]

    def start(self):
        for copy in self.direct():
            copy.start()

    def relays(self):
        return [
            self.copy(self.across, 0, 4, self.along),
            self.copy(self.along, 1, 5, self.across),
        ]

    def arrive(self, owner, piece):
        self.copy(owner, piece, 0, self.across if self.relay else owner).wait_recv()

    def pass_on(self):
        if self.relay:
            first, second = self.relays()
            self.arrive(self.across, 0)
            first.start()
            self.arrive(self.along, 1)
            second.start()

    def finish_near(self):
        if self.relay:
            self.arrive(self.across, 1)
            self.arrive(self.along, 0)

    def finish(self):
        if self.relay:
            far = 3 - self.tp
            self.arrive(far, 0)
            self.arrive(far, 1)
        else:
            for j in range(1, self.n_tp):
                self.arrive(lax.rem(self.tp + j, self.n_tp), 0)

    def sent(self):
        for copy in self.direct() + (self.relays() if self.relay else []):
            copy.wait_send()


def layer_kernel(
    n_sp,
    n_tp,
    residual,
    pool_in,
    docs,
    pool_weight,
    pool_gain,
    norm_gain,
    routes,
    route_weights,
    wout_hbm,
    gate_hbm,
    up_hbm,
    down_hbm,
    out,
    ext,
    halo,
    halo_docs,
    gathered,
    acc,
    mine,
    sums,
    send,
    rows,
    act,
    prod,
    ret,
    wout,
    w_gate,
    w_up,
    w_down,
    load_sem,
    h_send,
    h_recv,
    p_send,
    p_recv,
    s_send,
    s_recv,
    d_send,
    d_recv,
    f_send,
    f_recv,
    a_send,
    a_recv,
    r_send,
    r_recv,
):
    sp, tp = lax.axis_index("sp"), lax.axis_index("tp")
    chips = n_sp // CORES
    my_chip, my_core = sp // CORES, sp % CORES
    length, width = pool_in.shape
    cols = residual.shape[1]
    cap = send.shape[2]
    hidden = act.shape[4]
    flat = CORES * cap
    experts = n_sp
    relay = n_tp == 4

    loads = [
        pltpu.make_async_copy(wout_hbm, wout, load_sem.at[0]),
        pltpu.make_async_copy(gate_hbm, w_gate, load_sem.at[1]),
        pltpu.make_async_copy(up_hbm, w_up, load_sem.at[2]),
        pltpu.make_async_copy(down_hbm, w_down, load_sem.at[3]),
    ]
    for copy in loads:
        copy.start()

    barrier = pltpu.get_barrier_semaphore()
    peers = [(lax.rem(sp + j, n_sp), tp) for j in range(1, n_sp)]
    peers += [(sp, lax.rem(tp + j, n_tp)) for j in range(1, n_tp)]
    for device in peers:
        pl.semaphore_signal(barrier, inc=1, device_id=device, device_id_type=MESH)

    high = max(16, experts)
    route = [routes[k : k + 1, :] for k in range(TOPK)]
    expert = lax.broadcasted_iota(jnp.int32, (high, length), 0)
    used = sum((expert == route[k]).astype(jnp.float32) for k in range(TOPK))
    before = lax.broadcasted_iota(jnp.int32, (length, length), 0) < lax.broadcasted_iota(
        jnp.int32, (length, length), 1
    )
    taken = jnp.dot(
        used.astype(jnp.bfloat16), before.astype(jnp.bfloat16), preferred_element_type=jnp.float32
    )
    slot = []
    for k in range(TOPK):
        rank = jnp.sum(jnp.where(expert == route[k], taken, 0.0), axis=0, keepdims=True)
        slot.append(route[k].astype(jnp.float32) * cap + rank)
    doc_row = docs[...].astype(jnp.float32)
    line = lax.broadcasted_iota(jnp.int32, (LANES, length), 0)
    table = jnp.where(line == 0, doc_row, 0.0)
    for k in range(TOPK):
        table = jnp.where(line == 1 + k, slot[k], table)
        table = jnp.where(line == 1 + TOPK + k, route_weights[k : k + 1, :], table)
    columns = table.T
    doc_column = columns[:, 0:1]
    slot_column = [columns[:, 1 + k : 2 + k] for k in range(TOPK)]
    weight_column = [columns[:, 1 + TOPK + k : 2 + TOPK + k] for k in range(TOPK)]

    ext[0 : LANES - TAIL, :] = jnp.zeros((LANES - TAIL, width), jnp.bfloat16)
    ext[LANES:, :] = pool_in[...]

    pl.semaphore_wait(barrier, len(peers))

    following = (lax.rem(sp + 1, n_sp), tp)
    halo_copies = [
        remote(docs.at[:, length - LANES :], halo_docs, h_send.at[0], h_recv.at[0], following),
        remote(pool_in.at[length - TAIL :, :], halo, h_send.at[1], h_recv.at[1], following),
    ]
    for copy in halo_copies:
        copy.start()

    blocks = length // LANES
    away = (
        LANES
        + lax.broadcasted_iota(jnp.int32, (LANES, 2 * LANES), 0)
        - lax.broadcasted_iota(jnp.int32, (LANES, 2 * LANES), 1)
    )
    half = LANES // 2

    def pooled_spread(b):
        def block(owner, piece):
            if relay:
                return gathered.at[owner, pl.ds(b * LANES + piece * half, half), :]
            return gathered.at[owner, pl.ds(b * LANES, LANES), :]

        return Spread(
            n_tp, sp, tp, block, lambda i: p_send.at[b, i], lambda owner, piece: p_recv.at[b, owner, piece]
        )

    def pool(b, prior):
        low = b * LANES
        near = (doc_column[low : low + LANES, :] == prior) & (away >= 0)
        groups = width // GD
        for g in range(groups):
            if groups % 4 == 0:
                span = 2 << (g % 4)
            else:
                span = lax.shift_left(jnp.int32(2), (tp * groups + g) % 4)
            weight = (near & (away < span)).astype(jnp.float32)
            at = slice(g * GD, (g + 1) * GD)
            count = jnp.sum(weight, axis=1, keepdims=True)
            total = jnp.dot(
                weight.astype(jnp.bfloat16), ext[low : low + 2 * LANES, at], preferred_element_type=jnp.float32
            )
            own = ext[low + LANES : low + 2 * LANES, at].astype(jnp.float32)
            diff = (total / count - own).astype(jnp.bfloat16)
            mixed = jnp.dot(diff, pool_weight[g], preferred_element_type=jnp.float32)
            gathered[tp, low : low + LANES, at] = (mixed * pool_gain[:, at]).astype(jnp.bfloat16)
        pooled_spread(b).start()

    for b in range(1, blocks):
        pool(b, doc_row[:, (b - 1) * LANES : (b + 1) * LANES])
    for copy in halo_copies:
        copy.wait_recv()
    ext[LANES - TAIL : LANES, :] = halo[...]
    first_docs = jnp.where(sp > 0, halo_docs[...].astype(jnp.float32), -1.0)
    pool(0, jnp.concatenate([first_docs, doc_row[:, :LANES]], axis=1))

    def part(owner):
        deep = pl.ds(pl.multiple_of(owner * width, width), width)
        return jnp.dot(gathered[owner], wout[deep, :], preferred_element_type=jnp.float32)

    loads[0].wait()
    acc[...] = residual[...].astype(jnp.float32) + part(tp)
    order = list(range(1, blocks)) + [0]
    for b in order:
        pooled_spread(b).pass_on()
    if relay:
        for b in order:
            pooled_spread(b).finish_near()
        acc[...] += part(2 * (tp // 2) + 1 - tp % 2)
        acc[...] += part((tp + 2) % 4)
        for b in order:
            pooled_spread(b).finish()
        acc[...] += part(3 - tp)
    else:
        for b in order:
            pooled_spread(b).finish()

        @pl.loop(1, n_tp)
        def _(j):
            acc[...] += part(lax.rem(tp + j, n_tp))

    upf = acc[...].astype(jnp.bfloat16).astype(jnp.float32)
    acc[...] = upf
    squares = jnp.sum(upf * upf, axis=1, keepdims=True)
    own = jnp.broadcast_to(squares, (length, LANES)).T[0:8]
    mine[...] = own
    small = [
        remote(mine, sums.at[tp], s_send.at[j - 1], s_recv.at[tp], (sp, lax.rem(tp + j, n_tp)))
        for j in range(1, n_tp)
    ]
    for copy in small:
        copy.start()
    for j in range(1, n_tp):
        owner = lax.rem(tp + n_tp - j, n_tp)
        remote(mine, sums.at[owner], s_send.at[0], s_recv.at[owner], (sp, owner)).wait_recv()
        own = own + sums[owner]
    scale = lax.rsqrt(own / (cols * n_tp) + EPS)
    column = jnp.broadcast_to(scale[0:1], (LANES, length)).T[:, 0:1]
    gain = norm_gain[:, pl.ds(pl.multiple_of(tp * cols, LANES), cols)]
    normed = (acc[...] * column * gain).astype(jnp.bfloat16)

    step = 1 - 2 * (my_chip // ((chips + 1) // 2))

    def source(k):
        return (my_chip + step * k + chips) % chips

    def dispatch(chip, core):
        return remote(
            send.at[chip, core],
            rows.at[my_chip, tp, my_core],
            d_send.at[chip * CORES + core],
            d_recv.at[sp],
            (chip * CORES + core, tp),
        )

    place = lax.broadcasted_iota(jnp.int32, (flat, length), 0).astype(jnp.float32)
    for k in range(chips):
        chip = source(k)
        here = place + (chip * flat).astype(jnp.float32)
        pick = sum((here == slot[j]).astype(jnp.float32) for j in range(TOPK)).astype(jnp.bfloat16)
        chosen = jnp.dot(pick, normed, preferred_element_type=jnp.float32).astype(jnp.bfloat16)
        send[chip] = chosen.reshape(CORES, cap, cols)
        if k == 0:
            rows[my_chip, tp, my_core] = send[my_chip, my_core]
            dispatch(my_chip, 1 - my_core).start()
        else:
            for core in range(CORES):
                dispatch(chip, core).start()

    def spread_of(buf, ssem, rsem, chip):
        def block(owner, piece):
            return buf.at[chip, owner, piece] if relay else buf.at[chip, owner]

        return Spread(
            n_tp, sp, tp, block, lambda i: ssem.at[chip, i], lambda owner, piece: rsem.at[chip, owner, piece]
        )

    def row_spread(chip):
        return spread_of(rows, f_send, f_recv, chip)

    def act_spread(chip):
        return spread_of(act, a_send, a_recv, chip)

    def give_back(chip, core):
        return remote(
            prod.at[chip, core],
            ret.at[my_chip, my_core],
            r_send.at[chip * CORES + core],
            r_recv.at[sp],
            (chip * CORES + core, tp),
        )

    tile = min(hidden, 256)
    wide = min(cols, 256)

    def activate(chip):
        @pl.loop(0, hidden // tile)
        def _(n):
            at = pl.ds(pl.multiple_of(n * tile, tile), tile)
            gate = jnp.zeros((flat, tile), jnp.float32)
            up = jnp.zeros((flat, tile), jnp.float32)
            for t in range(n_tp):
                block = rows[chip, t].reshape(flat, cols)
                deep = pl.ds(t * cols, cols)
                gate += jnp.dot(block, w_gate[deep, at], preferred_element_type=jnp.float32)
                up += jnp.dot(block, w_up[deep, at], preferred_element_type=jnp.float32)
            value = (jax.nn.silu(gate) * up).astype(jnp.bfloat16)
            act[chip, tp, :, :, at] = value.reshape(CORES, cap, tile)

    def produce(chip):
        @pl.loop(0, cols // wide)
        def _(n):
            at = pl.ds(pl.multiple_of(n * wide, wide), wide)
            total = jnp.zeros((flat, wide), jnp.float32)
            for t in range(n_tp):
                block = act[chip, t].reshape(flat, hidden)
                deep = pl.ds(t * hidden, hidden)
                total += jnp.dot(block, w_down[deep, at], preferred_element_type=jnp.float32)
            prod[chip, :, :, at] = total.astype(jnp.bfloat16).reshape(CORES, cap, wide)

    @pl.loop(0, chips + 2)
    def _(i):
        @pl.when(i < chips)
        def _():
            chip = source(i)
            for core in range(CORES):

                @pl.when(chip * CORES + core != sp)
                def _():
                    remote(
                        send.at[chip, core],
                        rows.at[chip, tp, core],
                        d_send.at[0],
                        d_recv.at[chip * CORES + core],
                        (chip * CORES + core, tp),
                    ).wait_recv()

            row_spread(chip).start()

        @pl.when(i == chips)
        def _():
            act_spread(my_chip).start()

        @pl.when(i == 1)
        def _():
            for copy in loads[1:]:
                copy.wait()

        @pl.when((i >= 1) & (i < chips + 1))
        def _():
            chip = source(i - 1)
            row_spread(chip).finish_near()
            row_spread(chip).finish()
            activate(chip)

            @pl.when(i >= 2)
            def _():
                act_spread(chip).start()

        @pl.when(i >= 3)
        def _():
            chip = source(i - 2)
            act_spread(chip).finish_near()
            act_spread(chip).finish()
            produce(chip)
            for core in range(CORES):
                give_back(chip, core).start()

        @pl.when(i < chips)
        def _():
            row_spread(source(i)).pass_on()

        @pl.when(i == chips)
        def _():
            act_spread(my_chip).pass_on()

        @pl.when((i >= 2) & (i < chips + 1))
        def _():
            act_spread(source(i - 1)).pass_on()

    act_spread(my_chip).finish_near()
    act_spread(my_chip).finish()
    produce(my_chip)
    give_back(my_chip, 1 - my_core).start()
    ret[my_chip, my_core] = prod[my_chip, my_core]

    lane = lax.broadcasted_iota(jnp.int32, (length, flat), 1).astype(jnp.float32)
    late = [k for k in range(1, chips) if k != chips // 2]
    for k in [chips // 2, 0] + late if chips > 1 else [0]:
        chip = source(k)
        here = lane + (chip * flat).astype(jnp.float32)
        weight = sum(
            jnp.where(slot_column[j] == here, weight_column[j], 0.0) for j in range(TOPK)
        )
        upper = weight.astype(jnp.bfloat16)
        lower = (weight - upper.astype(jnp.float32)).astype(jnp.bfloat16)
        for core in range(CORES):

            @pl.when(chip * CORES + core != sp)
            def _():
                remote(
                    prod.at[chip, core],
                    ret.at[chip, core],
                    r_send.at[0],
                    r_recv.at[chip * CORES + core],
                    (chip * CORES + core, tp),
                ).wait_recv()

        back = ret[chip].reshape(flat, cols)
        acc[...] += jnp.dot(upper, back, preferred_element_type=jnp.float32) + jnp.dot(
            lower, back, preferred_element_type=jnp.float32
        )
    out[...] = acc[...].astype(jnp.bfloat16)

    for copy in halo_copies + small:
        copy.wait_send()
    for b in range(blocks):
        pooled_spread(b).sent()
    dispatch(my_chip, 1 - my_core).wait_send()
    give_back(my_chip, 1 - my_core).wait_send()

    @pl.loop(1, chips)
    def _(k):
        for core in range(CORES):
            dispatch(source(k), core).wait_send()
            give_back(source(k), core).wait_send()

    @pl.loop(0, chips)
    def _(chip):
        row_spread(chip).sent()
        act_spread(chip).sent()


def shards(
    residual,
    pool_in,
    docs,
    pool_weight,
    pool_gain,
    out_weight,
    norm_gain,
    routes,
    route_weights,
    w_gate,
    w_up,
    w_down,
):
    length, width = pool_in.shape
    cols = residual.shape[1]
    hidden = w_gate.shape[2]
    n_sp, n_tp = lax.axis_size("sp"), lax.axis_size("tp")
    chips = n_sp // CORES
    cap = length * TOPK * 3 // (2 * n_sp)
    blocks = length // LANES
    pieces = 2 if n_tp == 4 else 1
    fan = 6 if n_tp == 4 else n_tp
    dma = pltpu.SemaphoreType.DMA
    vmem = pl.BlockSpec(memory_space=pltpu.VMEM)
    hbm = pl.BlockSpec(memory_space=pl.ANY)
    half = jnp.bfloat16
    return pl.pallas_call(
        functools.partial(layer_kernel, n_sp, n_tp),
        out_shape=jax.ShapeDtypeStruct((length, cols), half),
        in_specs=[vmem] * 8 + [hbm] * 4,
        out_specs=vmem,
        scratch_shapes=[
            pltpu.VMEM((LANES + length, width), half),
            pltpu.VMEM((TAIL, width), half),
            pltpu.VMEM((1, LANES), jnp.int32),
            pltpu.VMEM((n_tp, length, width), half),
            pltpu.VMEM((length, cols), jnp.float32),
            pltpu.VMEM((8, length), jnp.float32),
            pltpu.VMEM((n_tp, 8, length), jnp.float32),
            pltpu.VMEM((chips, CORES, cap, cols), half),
            pltpu.VMEM((chips, n_tp, CORES, cap, cols), half),
            pltpu.VMEM((chips, n_tp, CORES, cap, hidden), half),
            pltpu.VMEM((chips, CORES, cap, cols), half),
            pltpu.VMEM((chips, CORES, cap, cols), half),
            pltpu.VMEM(out_weight.shape, half),
            pltpu.VMEM(w_gate.shape[1:], half),
            pltpu.VMEM(w_up.shape[1:], half),
            pltpu.VMEM(w_down.shape[1:], half),
            dma((4,)),
            dma((2,)),
            dma((2,)),
            dma((blocks, fan)),
            dma((blocks, n_tp, pieces)),
            dma((n_tp,)),
            dma((n_tp,)),
            dma((n_sp,)),
            dma((n_sp,)),
            dma((chips, fan)),
            dma((chips, n_tp, pieces)),
            dma((chips, fan)),
            dma((chips, n_tp, pieces)),
            dma((n_sp,)),
            dma((n_sp,)),
        ],
        compiler_params=pltpu.CompilerParams(
            collective_id=0, has_side_effects=True, vmem_limit_bytes=VMEM_LIMIT
        ),
    )(
        residual,
        pool_in,
        docs.reshape(1, length),
        pool_weight,
        pool_gain.reshape(1, width),
        norm_gain.reshape(1, -1),
        routes.T,
        route_weights.T,
        out_weight,
        w_gate[0],
        w_up[0],
        w_down[0],
    )


def solution(mesh):
    placed = (
        P("sp", "tp"),
        P("sp", "tp"),
        P("sp"),
        P("tp", None, None),
        P("tp"),
        P(None, "tp"),
        P(),
        P("sp", None),
        P("sp", None),
        P("sp", None, "tp"),
        P("sp", None, "tp"),
        P("sp", None, "tp"),
    )
    return jax.shard_map(
        shards, mesh=mesh, in_specs=placed, out_specs=P("sp", "tp"), check_vma=False
    )
```

```python
import functools

import jax
import jax.numpy as jnp
from jax import lax
from jax.experimental import pallas as pl
from jax.experimental.pallas import tpu as pltpu
from jax.sharding import PartitionSpec as P

GD = 128
TOPK = 2
EPS = 1e-06
MESH = pl.DeviceIdType.MESH
CORES = 2
LANES = 128
TAIL = 16
VMEM_LIMIT = 62 * 1024 * 1024


def remote(src, dst, send_sem, recv_sem, device):
    return pltpu.make_async_remote_copy(
        src_ref=src,
        dst_ref=dst,
        send_sem=send_sem,
        recv_sem=recv_sem,
        device_id=device,
        device_id_type=MESH,
    )


class Spread:
    def __init__(self, n_tp, sp, tp, block, send_sem, recv_sem):
        self.n_tp, self.sp, self.tp = n_tp, sp, tp
        self.block, self.send_sem, self.recv_sem = block, send_sem, recv_sem
        self.relay = n_tp == 4
        self.across = 2 * (tp // 2) + 1 - tp % 2
        self.along = (tp + 2) % 4

    def copy(self, owner, piece, sem, peer):
        ref = self.block(owner, piece)
        return remote(ref, ref, self.send_sem(sem), self.recv_sem(owner, piece), (self.sp, peer))

    def direct(self):
        if self.relay:
            return [
                self.copy(self.tp, 0, 0, self.across),
                self.copy(self.tp, 1, 1, self.along),
                self.copy(self.tp, 1, 2, self.across),
                self.copy(self.tp, 0, 3, self.along),
            ]
        return [
            self.copy(self.tp, 0, j - 1, lax.rem(self.tp + j, self.n_tp)) for j in range(1, self.n_tp)
        ]

    def start(self):
        for copy in self.direct():
            copy.start()

    def relays(self):
        return [
            self.copy(self.across, 0, 4, self.along),
            self.copy(self.along, 1, 5, self.across),
        ]

    def arrive(self, owner, piece):
        self.copy(owner, piece, 0, self.across if self.relay else owner).wait_recv()

    def pass_on(self):
        if self.relay:
            first, second = self.relays()
            self.arrive(self.across, 0)
            first.start()
            self.arrive(self.along, 1)
            second.start()

    def finish_near(self):
        if self.relay:
            self.arrive(self.across, 1)
            self.arrive(self.along, 0)

    def finish(self):
        if self.relay:
            far = 3 - self.tp
            self.arrive(far, 0)
            self.arrive(far, 1)
        else:
            for j in range(1, self.n_tp):
                self.arrive(lax.rem(self.tp + j, self.n_tp), 0)

    def sent(self):
        for copy in self.direct() + (self.relays() if self.relay else []):
            copy.wait_send()


STAGES = ["D", "RD", "CD", "A", "RA", "CA"]
MID = (
    "D0 RD0 D3 RD3",
    "D1 CD3 A3 RA3",
    "D2 CA3 RD2 RD1",
    "CD0 CD2 A2 RA2",
    "CD1 A1 CA2 RA1",
    "A0 CA1 RA0 CA0",
)
EDGE = (
    "D0 RD0 D1 RD1",
    "D3 CD1 RD3 D2",
    "CD3 A3 RA3 CD0",
    "A1 RD2 CA3 RA1",
    "CD2 A2 CA1 RA2",
    "CA2 A0 RA0 CA0",
)


def schedules(chips):
    if chips == 4:
        return [[(step[:-1], int(step[-1])) for step in " ".join(plan).split()] for plan in (MID, EDGE)]
    steps = [("D", 0), ("RD", 0)]
    for k in range(1, chips):
        steps += [("D", k), ("RD", k), ("CD", k - 1), ("A", k - 1), ("RA", k - 1), ("CA", k - 1)]
    last = chips - 1
    steps += [("CD", last), ("A", last), ("RA", last), ("CA", last)]
    return steps, steps


def send_order(chips):
    return [0, 1, 3, 2] if chips == 4 else list(range(chips))


def return_orders(chips):
    if chips == 4:
        return [3, 2, 0, 1], [3, 1, 0, 2]
    return [list(range(1, chips)) + [0]] * 2


def layer_kernel(
    n_sp,
    n_tp,
    residual,
    pool_in,
    docs,
    pool_weight,
    pool_gain,
    norm_gain,
    routes,
    route_weights,
    wout_hbm,
    gate_hbm,
    up_hbm,
    down_hbm,
    out,
    ext,
    halo,
    halo_docs,
    gathered,
    acc,
    mine,
    sums,
    send,
    rows,
    act,
    prod,
    ret,
    wout,
    w_gate,
    w_up,
    w_down,
    load_sem,
    h_send,
    h_recv,
    p_send,
    p_recv,
    s_send,
    s_recv,
    d_send,
    d_recv,
    f_send,
    f_recv,
    a_send,
    a_recv,
    r_send,
    r_recv,
):
    sp, tp = lax.axis_index("sp"), lax.axis_index("tp")
    chips = n_sp // CORES
    my_chip, my_core = sp // CORES, sp % CORES
    length, width = pool_in.shape
    cols = residual.shape[1]
    cap = send.shape[2]
    hidden = act.shape[4]
    flat = CORES * cap
    experts = n_sp
    relay = n_tp == 4

    loads = [
        pltpu.make_async_copy(wout_hbm, wout, load_sem.at[0]),
        pltpu.make_async_copy(gate_hbm, w_gate, load_sem.at[1]),
        pltpu.make_async_copy(up_hbm, w_up, load_sem.at[2]),
        pltpu.make_async_copy(down_hbm, w_down, load_sem.at[3]),
    ]
    for copy in loads:
        copy.start()

    barrier = pltpu.get_barrier_semaphore()
    peers = [(lax.rem(sp + j, n_sp), tp) for j in range(1, n_sp)]
    peers += [(sp, lax.rem(tp + j, n_tp)) for j in range(1, n_tp)]
    for device in peers:
        pl.semaphore_signal(barrier, inc=1, device_id=device, device_id_type=MESH)

    high = max(16, experts)
    route = [routes[k : k + 1, :] for k in range(TOPK)]
    expert = lax.broadcasted_iota(jnp.int32, (high, length), 0)
    used = sum((expert == route[k]).astype(jnp.float32) for k in range(TOPK))
    before = lax.broadcasted_iota(jnp.int32, (length, length), 0) < lax.broadcasted_iota(
        jnp.int32, (length, length), 1
    )
    taken = jnp.dot(
        used.astype(jnp.bfloat16), before.astype(jnp.bfloat16), preferred_element_type=jnp.float32
    )
    slot = []
    for k in range(TOPK):
        rank = jnp.sum(jnp.where(expert == route[k], taken, 0.0), axis=0, keepdims=True)
        slot.append(route[k].astype(jnp.float32) * cap + rank)
    doc_row = docs[...].astype(jnp.float32)
    line = lax.broadcasted_iota(jnp.int32, (LANES, length), 0)
    table = jnp.where(line == 0, doc_row, 0.0)
    for k in range(TOPK):
        table = jnp.where(line == 1 + k, slot[k], table)
        table = jnp.where(line == 1 + TOPK + k, route_weights[k : k + 1, :], table)
    columns = table.T
    doc_column = columns[:, 0:1]
    slot_column = [columns[:, 1 + k : 2 + k] for k in range(TOPK)]
    weight_column = [columns[:, 1 + TOPK + k : 2 + TOPK + k] for k in range(TOPK)]

    ext[0 : LANES - TAIL, :] = jnp.zeros((LANES - TAIL, width), jnp.bfloat16)
    ext[LANES:, :] = pool_in[...]

    pl.semaphore_wait(barrier, len(peers))

    following = (lax.rem(sp + 1, n_sp), tp)
    halo_copies = [
        remote(docs.at[:, length - LANES :], halo_docs, h_send.at[0], h_recv.at[0], following),
        remote(pool_in.at[length - TAIL :, :], halo, h_send.at[1], h_recv.at[1], following),
    ]
    for copy in halo_copies:
        copy.start()

    blocks = length // LANES
    away = (
        LANES
        + lax.broadcasted_iota(jnp.int32, (LANES, 2 * LANES), 0)
        - lax.broadcasted_iota(jnp.int32, (LANES, 2 * LANES), 1)
    )
    half = LANES // 2

    def pooled_spread(b):
        def block(owner, piece):
            if relay:
                return gathered.at[owner, pl.ds(b * LANES + piece * half, half), :]
            return gathered.at[owner, pl.ds(b * LANES, LANES), :]

        return Spread(
            n_tp, sp, tp, block, lambda i: p_send.at[b, i], lambda owner, piece: p_recv.at[b, owner, piece]
        )

    def pool(b, prior):
        low = b * LANES
        near = (doc_column[low : low + LANES, :] == prior) & (away >= 0)
        groups = width // GD
        for g in range(groups):
            if groups % 4 == 0:
                span = 2 << (g % 4)
            else:
                span = lax.shift_left(jnp.int32(2), (tp * groups + g) % 4)
            weight = (near & (away < span)).astype(jnp.float32)
            at = slice(g * GD, (g + 1) * GD)
            count = jnp.sum(weight, axis=1, keepdims=True)
            total = jnp.dot(
                weight.astype(jnp.bfloat16), ext[low : low + 2 * LANES, at], preferred_element_type=jnp.float32
            )
            own = ext[low + LANES : low + 2 * LANES, at].astype(jnp.float32)
            diff = (total / count - own).astype(jnp.bfloat16)
            mixed = jnp.dot(diff, pool_weight[g], preferred_element_type=jnp.float32)
            gathered[tp, low : low + LANES, at] = (mixed * pool_gain[:, at]).astype(jnp.bfloat16)
        pooled_spread(b).start()

    for b in range(1, blocks):
        pool(b, doc_row[:, (b - 1) * LANES : (b + 1) * LANES])
    for copy in halo_copies:
        copy.wait_recv()
    ext[LANES - TAIL : LANES, :] = halo[...]
    first_docs = jnp.where(sp > 0, halo_docs[...].astype(jnp.float32), -1.0)
    pool(0, jnp.concatenate([first_docs, doc_row[:, :LANES]], axis=1))

    def part(owner):
        deep = pl.ds(pl.multiple_of(owner * width, width), width)
        return jnp.dot(gathered[owner], wout[deep, :], preferred_element_type=jnp.float32)

    loads[0].wait()
    acc[...] = residual[...].astype(jnp.float32) + part(tp)
    order = list(range(1, blocks)) + [0]
    for b in order:
        pooled_spread(b).pass_on()
    if relay:
        for b in order:
            pooled_spread(b).finish_near()
        acc[...] += part(2 * (tp // 2) + 1 - tp % 2)
        acc[...] += part((tp + 2) % 4)
        for b in order:
            pooled_spread(b).finish()
        acc[...] += part(3 - tp)
    else:
        for b in order:
            pooled_spread(b).finish()

        @pl.loop(1, n_tp)
        def _(j):
            acc[...] += part(lax.rem(tp + j, n_tp))

    upf = acc[...].astype(jnp.bfloat16).astype(jnp.float32)
    acc[...] = upf
    squares = jnp.sum(upf * upf, axis=1, keepdims=True)
    own = jnp.broadcast_to(squares, (length, LANES)).T[0:8]
    mine[...] = own
    small = [
        remote(mine, sums.at[tp], s_send.at[j - 1], s_recv.at[tp], (sp, lax.rem(tp + j, n_tp)))
        for j in range(1, n_tp)
    ]
    for copy in small:
        copy.start()
    for j in range(1, n_tp):
        owner = lax.rem(tp + n_tp - j, n_tp)
        remote(mine, sums.at[owner], s_send.at[0], s_recv.at[owner], (sp, owner)).wait_recv()
        own = own + sums[owner]
    scale = lax.rsqrt(own / (cols * n_tp) + EPS)
    column = jnp.broadcast_to(scale[0:1], (LANES, length)).T[:, 0:1]
    gain = norm_gain[:, pl.ds(pl.multiple_of(tp * cols, LANES), cols)]
    normed = (acc[...] * column * gain).astype(jnp.bfloat16)

    def source(k):
        bits = range(max(1, (chips - 1).bit_length()))
        return sum(((my_chip // 2**b + k // 2**b) % 2) * 2**b for b in bits)

    inner = ((my_chip + 1) // 2) % 2

    def pick_by(i, mid, edge):
        value = 0
        for at, (a, b) in enumerate(zip(mid, edge)):
            value = value + jnp.where(i == at, b + (a - b) * inner, 0)
        return value

    def dispatch(chip, core):
        return remote(
            send.at[chip, core],
            rows.at[my_chip, tp, my_core],
            d_send.at[chip * CORES + core],
            d_recv.at[sp],
            (chip * CORES + core, tp),
        )

    place = lax.broadcasted_iota(jnp.int32, (flat, length), 0).astype(jnp.float32)
    for k in send_order(chips):
        chip = source(k)
        here = place + (chip * flat).astype(jnp.float32)
        pick = sum((here == slot[j]).astype(jnp.float32) for j in range(TOPK)).astype(jnp.bfloat16)
        chosen = jnp.dot(pick, normed, preferred_element_type=jnp.float32).astype(jnp.bfloat16)
        send[chip] = chosen.reshape(CORES, cap, cols)
        if k == 0:
            rows[my_chip, tp, my_core] = send[my_chip, my_core]
            dispatch(my_chip, 1 - my_core).start()
        else:
            for core in range(CORES):
                dispatch(chip, core).start()

    def spread_of(buf, ssem, rsem, chip):
        def block(owner, piece):
            return buf.at[chip, owner, piece] if relay else buf.at[chip, owner]

        return Spread(
            n_tp, sp, tp, block, lambda i: ssem.at[chip, i], lambda owner, piece: rsem.at[chip, owner, piece]
        )

    def row_spread(chip):
        return spread_of(rows, f_send, f_recv, chip)

    def act_spread(chip):
        return spread_of(act, a_send, a_recv, chip)

    def give_back(chip, core):
        return remote(
            prod.at[chip, core],
            ret.at[my_chip, my_core],
            r_send.at[chip * CORES + core],
            r_recv.at[sp],
            (chip * CORES + core, tp),
        )

    tile = min(hidden, 256)
    wide = min(cols, 256)

    def activate(chip):
        @pl.loop(0, hidden // tile)
        def _(n):
            at = pl.ds(pl.multiple_of(n * tile, tile), tile)
            gate = jnp.zeros((flat, tile), jnp.float32)
            up = jnp.zeros((flat, tile), jnp.float32)
            for t in range(n_tp):
                block = rows[chip, t].reshape(flat, cols)
                deep = pl.ds(t * cols, cols)
                gate += jnp.dot(block, w_gate[deep, at], preferred_element_type=jnp.float32)
                up += jnp.dot(block, w_up[deep, at], preferred_element_type=jnp.float32)
            value = (jax.nn.silu(gate) * up).astype(jnp.bfloat16)
            act[chip, tp, :, :, at] = value.reshape(CORES, cap, tile)

    def produce(chip):
        @pl.loop(0, cols // wide)
        def _(n):
            at = pl.ds(pl.multiple_of(n * wide, wide), wide)
            total = jnp.zeros((flat, wide), jnp.float32)
            for t in range(n_tp):
                block = act[chip, t].reshape(flat, hidden)
                deep = pl.ds(t * hidden, hidden)
                total += jnp.dot(block, w_down[deep, at], preferred_element_type=jnp.float32)
            prod[chip, :, :, at] = total.astype(jnp.bfloat16).reshape(CORES, cap, wide)

    def start_rows(chip):
        for core in range(CORES):

            @pl.when(chip * CORES + core != sp)
            def _():
                remote(
                    send.at[chip, core],
                    rows.at[chip, tp, core],
                    d_send.at[0],
                    d_recv.at[chip * CORES + core],
                    (chip * CORES + core, tp),
                ).wait_recv()

        row_spread(chip).start()

    def finish_rows(chip):
        row_spread(chip).finish_near()
        row_spread(chip).finish()
        activate(chip)

    def finish_act(chip):
        act_spread(chip).finish_near()
        act_spread(chip).finish()
        produce(chip)
        for core in range(CORES):

            @pl.when(chip * CORES + core != sp)
            def _():
                give_back(chip, core).start()

        @pl.when(chip == my_chip)
        def _():
            ret[my_chip, my_core] = prod[my_chip, my_core]

    stages = [
        start_rows,
        lambda chip: row_spread(chip).pass_on(),
        finish_rows,
        lambda chip: act_spread(chip).start(),
        lambda chip: act_spread(chip).pass_on(),
        finish_act,
    ]
    mid, edge = [
        [STAGES.index(name) * chips + k for name, k in steps] for steps in schedules(chips)
    ]
    for copy in loads[1:]:
        copy.wait()

    @pl.loop(0, len(mid))
    def _(i):
        code = pick_by(i, mid, edge)
        chip = source(code % chips)
        for at, stage in enumerate(stages):

            @pl.when(code // chips == at)
            def _():
                stage(chip)

    lane = lax.broadcasted_iota(jnp.int32, (length, flat), 1).astype(jnp.float32)
    orders = return_orders(chips)

    @pl.loop(0, chips)
    def _(i):
        chip = source(pick_by(i, *orders))
        here = lane + (chip * flat).astype(jnp.float32)
        weight = sum(
            jnp.where(slot_column[j] == here, weight_column[j], 0.0) for j in range(TOPK)
        )
        upper = weight.astype(jnp.bfloat16)
        lower = (weight - upper.astype(jnp.float32)).astype(jnp.bfloat16)
        for core in range(CORES):

            @pl.when(chip * CORES + core != sp)
            def _():
                remote(
                    prod.at[chip, core],
                    ret.at[chip, core],
                    r_send.at[0],
                    r_recv.at[chip * CORES + core],
                    (chip * CORES + core, tp),
                ).wait_recv()

        back = ret[chip].reshape(flat, cols)
        acc[...] += jnp.dot(upper, back, preferred_element_type=jnp.float32) + jnp.dot(
            lower, back, preferred_element_type=jnp.float32
        )
    out[...] = acc[...]

    for copy in halo_copies + small:
        copy.wait_send()
    for b in range(blocks):
        pooled_spread(b).sent()
    dispatch(my_chip, 1 - my_core).wait_send()
    give_back(my_chip, 1 - my_core).wait_send()

    @pl.loop(1, chips)
    def _(k):
        for core in range(CORES):
            dispatch(source(k), core).wait_send()
            give_back(source(k), core).wait_send()

    @pl.loop(0, chips)
    def _(chip):
        row_spread(chip).sent()
        act_spread(chip).sent()


def shards(
    residual,
    pool_in,
    docs,
    pool_weight,
    pool_gain,
    out_weight,
    norm_gain,
    routes,
    route_weights,
    w_gate,
    w_up,
    w_down,
):
    length, width = pool_in.shape
    cols = residual.shape[1]
    hidden = w_gate.shape[2]
    n_sp, n_tp = lax.axis_size("sp"), lax.axis_size("tp")
    chips = n_sp // CORES
    cap = length * TOPK * 3 // (2 * n_sp)
    blocks = length // LANES
    pieces = 2 if n_tp == 4 else 1
    fan = 6 if n_tp == 4 else n_tp
    dma = pltpu.SemaphoreType.DMA
    vmem = pl.BlockSpec(memory_space=pltpu.VMEM)
    hbm = pl.BlockSpec(memory_space=pl.ANY)
    half = jnp.bfloat16
    return pl.pallas_call(
        functools.partial(layer_kernel, n_sp, n_tp),
        out_shape=pltpu.VMEM((length, cols), jnp.float32),
        in_specs=[vmem] * 8 + [hbm] * 4,
        out_specs=vmem,
        scratch_shapes=[
            pltpu.VMEM((LANES + length, width), half),
            pltpu.VMEM((TAIL, width), half),
            pltpu.VMEM((1, LANES), jnp.int32),
            pltpu.VMEM((n_tp, length, width), half),
            pltpu.VMEM((length, cols), jnp.float32),
            pltpu.VMEM((8, length), jnp.float32),
            pltpu.VMEM((n_tp, 8, length), jnp.float32),
            pltpu.VMEM((chips, CORES, cap, cols), half),
            pltpu.VMEM((chips, n_tp, CORES, cap, cols), half),
            pltpu.VMEM((chips, n_tp, CORES, cap, hidden), half),
            pltpu.VMEM((chips, CORES, cap, cols), half),
            pltpu.VMEM((chips, CORES, cap, cols), half),
            pltpu.VMEM(out_weight.shape, half),
            pltpu.VMEM(w_gate.shape[1:], half),
            pltpu.VMEM(w_up.shape[1:], half),
            pltpu.VMEM(w_down.shape[1:], half),
            dma((4,)),
            dma((2,)),
            dma((2,)),
            dma((blocks, fan)),
            dma((blocks, n_tp, pieces)),
            dma((n_tp,)),
            dma((n_tp,)),
            dma((n_sp,)),
            dma((n_sp,)),
            dma((chips, fan)),
            dma((chips, n_tp, pieces)),
            dma((chips, fan)),
            dma((chips, n_tp, pieces)),
            dma((n_sp,)),
            dma((n_sp,)),
        ],
        compiler_params=pltpu.CompilerParams(
            collective_id=0, has_side_effects=True, vmem_limit_bytes=VMEM_LIMIT
        ),
    )(
        residual,
        pool_in,
        docs.reshape(1, length),
        pool_weight,
        pool_gain.reshape(1, width),
        norm_gain.reshape(1, -1),
        routes.T,
        route_weights.T,
        out_weight,
        w_gate[0],
        w_up[0],
        w_down[0],
    ).astype(half)


def solution(mesh):
    placed = (
        P("sp", "tp"),
        P("sp", "tp"),
        P("sp"),
        P("tp", None, None),
        P("tp"),
        P(None, "tp"),
        P(),
        P("sp", None),
        P("sp", None),
        P("sp", None, "tp"),
        P("sp", None, "tp"),
        P("sp", None, "tp"),
    )
    return jax.shard_map(
        shards, mesh=mesh, in_specs=placed, out_specs=P("sp", "tp"), check_vma=False
    )
```

```python
import functools

import jax
import jax.numpy as jnp
from jax import lax
from jax.experimental import pallas as pl
from jax.experimental.pallas import tpu as pltpu
from jax.sharding import PartitionSpec as P

GD = 128
TOPK = 2
EPS = 1e-06
MESH = pl.DeviceIdType.MESH
CORES = 2
LANES = 128
TAIL = 16
VMEM_LIMIT = 62 * 1024 * 1024


def remote(src, dst, send_sem, recv_sem, device):
    return pltpu.make_async_remote_copy(
        src_ref=src,
        dst_ref=dst,
        send_sem=send_sem,
        recv_sem=recv_sem,
        device_id=device,
        device_id_type=MESH,
    )


class Spread:
    def __init__(self, n_tp, sp, tp, block, send_sem, recv_sem):
        self.n_tp, self.sp, self.tp = n_tp, sp, tp
        self.block, self.send_sem, self.recv_sem = block, send_sem, recv_sem
        self.relay = n_tp == 4
        self.across = 2 * (tp // 2) + 1 - tp % 2
        self.along = (tp + 2) % 4

    def copy(self, owner, piece, sem, peer):
        ref = self.block(owner, piece)
        return remote(ref, ref, self.send_sem(sem), self.recv_sem(owner, piece), (self.sp, peer))

    def direct(self):
        if self.relay:
            return [
                self.copy(self.tp, 0, 0, self.across),
                self.copy(self.tp, 1, 1, self.along),
                self.copy(self.tp, 1, 2, self.across),
                self.copy(self.tp, 0, 3, self.along),
            ]
        return [
            self.copy(self.tp, 0, j - 1, lax.rem(self.tp + j, self.n_tp)) for j in range(1, self.n_tp)
        ]

    def start(self):
        for copy in self.direct():
            copy.start()

    def relays(self):
        return [
            self.copy(self.across, 0, 4, self.along),
            self.copy(self.along, 1, 5, self.across),
        ]

    def arrive(self, owner, piece):
        self.copy(owner, piece, 0, self.across if self.relay else owner).wait_recv()

    def pass_on(self):
        if self.relay:
            first, second = self.relays()
            self.arrive(self.across, 0)
            first.start()
            self.arrive(self.along, 1)
            second.start()

    def finish_near(self):
        if self.relay:
            self.arrive(self.across, 1)
            self.arrive(self.along, 0)

    def finish(self):
        if self.relay:
            far = 3 - self.tp
            self.arrive(far, 0)
            self.arrive(far, 1)
        else:
            for j in range(1, self.n_tp):
                self.arrive(lax.rem(self.tp + j, self.n_tp), 0)

    def sent(self):
        for copy in self.direct() + (self.relays() if self.relay else []):
            copy.wait_send()


STAGES = ["D", "RD", "CD", "A", "RA", "CA", "C", "Z"]
MID = (
    "RD0 Z0 D3 RD3",
    "D1 CD3 A3 RA3",
    "D2 CD0 CA3 RD2",
    "RD1 CD2 A2 CD1",
    "RA2 A1 CA2 RA1",
    "A0 C3 CA1 RA0",
    "C1 CA0 C0 C2",
)
EDGE = (
    "RD0 Z0 D1 CD0",
    "RD1 D3 RD3 D2",
    "CD3 CD1 A3 RA3",
    "RD2 A1 CA3 CD2",
    "RA1 A2 CA1 RA2",
    "A0 CA2 RA0 C3",
    "CA0 C2 C0 C1",
)


def schedules(chips):
    if chips == 4:
        return [[(step[:-1], int(step[-1])) for step in " ".join(plan).split()] for plan in (MID, EDGE)]
    steps = [("RD", 0)]
    for k in range(1, chips):
        steps += [("D", k), ("RD", k), ("CD", k - 1), ("A", k - 1), ("RA", k - 1), ("CA", k - 1)]
    last = chips - 1
    steps += [("CD", last), ("A", last), ("RA", last), ("CA", last)]
    steps += [("C", k) for k in range(chips)]
    return steps, steps


def send_order(chips):
    return ([0, 1], [3, 2]) if chips == 4 else (list(range(chips)), [])


def layer_kernel(
    n_sp,
    n_tp,
    residual_hbm,
    pool_in_hbm,
    docs_hbm,
    pool_weight_hbm,
    pool_gain_hbm,
    norm_gain_hbm,
    routes_hbm,
    route_weights_hbm,
    wout_hbm,
    gate_hbm,
    up_hbm,
    down_hbm,
    out,
    residual,
    pool_in,
    docs,
    pool_weight,
    pool_gain,
    norm_gain,
    routes,
    route_weights,
    ext,
    halo,
    halo_docs,
    gathered,
    acc,
    mine,
    sums,
    send,
    rows,
    act,
    prod,
    ret,
    scale_send,
    scale_rows,
    wout,
    w_gate,
    w_up,
    w_down,
    in_sem,
    load_sem,
    h_send,
    h_recv,
    p_send,
    p_recv,
    s_send,
    s_recv,
    d_send,
    d_recv,
    f_send,
    f_recv,
    a_send,
    a_recv,
    r_send,
    r_recv,
    e_send,
    e_recv,
    credit,
):
    sp, tp = lax.axis_index("sp"), lax.axis_index("tp")
    chips = n_sp // CORES
    my_chip, my_core = sp // CORES, sp % CORES
    length, width = pool_in.shape
    cols = residual.shape[1]
    cap = send.shape[2]
    hidden = act.shape[4]
    flat = CORES * cap
    experts = n_sp
    relay = n_tp == 4
    room = -(-cap // LANES) * LANES

    loads = [
        pltpu.make_async_copy(wout_hbm, wout, load_sem.at[0]),
        pltpu.make_async_copy(gate_hbm, w_gate, load_sem.at[1]),
        pltpu.make_async_copy(up_hbm, w_up, load_sem.at[2]),
        pltpu.make_async_copy(down_hbm, w_down, load_sem.at[3]),
    ]
    barrier = pltpu.get_barrier_semaphore()
    peers = [(lax.rem(sp + j, n_sp), tp) for j in range(1, n_sp)]
    peers += [(sp, lax.rem(tp + j, n_tp)) for j in range(1, n_tp)]
    for device in peers:
        pl.semaphore_signal(barrier, inc=1, device_id=device, device_id_type=MESH)
    inputs = [
        pltpu.make_async_copy(src, dst, in_sem.at[at])
        for at, (src, dst) in enumerate(
            (
                (routes_hbm, routes),
                (route_weights_hbm, route_weights),
                (docs_hbm, docs),
                (pool_in_hbm, pool_in),
                (pool_weight_hbm, pool_weight),
                (pool_gain_hbm, pool_gain),
                (norm_gain_hbm, norm_gain),
                (residual_hbm, residual),
            )
        )
    ]
    for copy in inputs:
        copy.start()
    for copy in inputs:
        copy.wait()
    for copy in loads:
        copy.start()

    high = max(16, experts)
    route = [routes[k : k + 1, :] for k in range(TOPK)]
    expert = lax.broadcasted_iota(jnp.int32, (high, length), 0)
    used = sum((expert == route[k]).astype(jnp.float32) for k in range(TOPK))
    before = lax.broadcasted_iota(jnp.int32, (length, length), 0) < lax.broadcasted_iota(
        jnp.int32, (length, length), 1
    )
    taken = jnp.dot(
        used.astype(jnp.bfloat16), before.astype(jnp.bfloat16), preferred_element_type=jnp.float32
    )
    slot = []
    for k in range(TOPK):
        rank = jnp.sum(jnp.where(expert == route[k], taken, 0.0), axis=0, keepdims=True)
        slot.append(route[k].astype(jnp.float32) * cap + rank)
    doc_row = docs[...].astype(jnp.float32)
    line = lax.broadcasted_iota(jnp.int32, (LANES, length), 0)
    table = jnp.where(line == 0, doc_row, 0.0)
    for k in range(TOPK):
        table = jnp.where(line == 1 + k, slot[k], table)
        table = jnp.where(line == 1 + TOPK + k, route_weights[k : k + 1, :], table)
    columns = table.T
    doc_column = columns[:, 0:1]
    slot_column = [columns[:, 1 + k : 2 + k] for k in range(TOPK)]
    weight_column = [columns[:, 1 + TOPK + k : 2 + TOPK + k] for k in range(TOPK)]

    ext[0 : LANES - TAIL, :] = jnp.zeros((LANES - TAIL, width), jnp.bfloat16)
    ext[LANES:, :] = pool_in[...]

    blocks = length // LANES
    away = (
        LANES
        + lax.broadcasted_iota(jnp.int32, (LANES, 2 * LANES), 0)
        - lax.broadcasted_iota(jnp.int32, (LANES, 2 * LANES), 1)
    )
    half = LANES // 2

    def pooled_spread(b):
        def block(owner, piece):
            if relay:
                return gathered.at[owner, pl.ds(b * LANES + piece * half, half), :]
            return gathered.at[owner, pl.ds(b * LANES, LANES), :]

        return Spread(
            n_tp, sp, tp, block, lambda i: p_send.at[b, i], lambda owner, piece: p_recv.at[b, owner, piece]
        )

    def pool(b, prior):
        low = b * LANES
        near = (doc_column[low : low + LANES, :] == prior) & (away >= 0)
        groups = width // GD
        for g in range(groups):
            if groups % 4 == 0:
                span = 2 << (g % 4)
            else:
                span = lax.shift_left(jnp.int32(2), (tp * groups + g) % 4)
            weight = (near & (away < span)).astype(jnp.float32)
            at = slice(g * GD, (g + 1) * GD)
            count = jnp.sum(weight, axis=1, keepdims=True)
            total = jnp.dot(
                weight.astype(jnp.bfloat16), ext[low : low + 2 * LANES, at], preferred_element_type=jnp.float32
            )
            own = ext[low + LANES : low + 2 * LANES, at].astype(jnp.float32)
            diff = (total / count - own).astype(jnp.bfloat16)
            mixed = jnp.dot(diff, pool_weight[g], preferred_element_type=jnp.float32)
            gathered[tp, low : low + LANES, at] = (mixed * pool_gain[:, at]).astype(jnp.bfloat16)

    for b in range(1, blocks):
        pool(b, doc_row[:, (b - 1) * LANES : (b + 1) * LANES])

    pl.semaphore_wait(barrier, len(peers))

    def halo_copies(to):
        return [
            remote(docs.at[:, length - LANES :], halo_docs, h_send.at[0], h_recv.at[0], (to, tp)),
            remote(pool_in.at[length - TAIL :, :], halo, h_send.at[1], h_recv.at[1], (to, tp)),
        ]

    @pl.when(sp < n_sp - 1)
    def _():
        for copy in halo_copies(sp + 1):
            copy.start()

    for b in range(1, blocks):
        pooled_spread(b).start()
    @pl.when(sp == 0)
    def _():
        halo[...] = jnp.zeros_like(halo)
        halo_docs[...] = jnp.full_like(halo_docs, -1)

    @pl.when(sp > 0)
    def _():
        for copy in halo_copies(sp - 1):
            copy.wait_recv()

    ext[LANES - TAIL : LANES, :] = halo[...]
    first_docs = halo_docs[...].astype(jnp.float32)
    pool(0, jnp.concatenate([first_docs, doc_row[:, :LANES]], axis=1))
    pooled_spread(0).start()

    def part(owner):
        deep = pl.ds(pl.multiple_of(owner * width, width), width)
        return jnp.dot(gathered[owner], wout[deep, :], preferred_element_type=jnp.float32)

    loads[0].wait()
    acc[...] = residual[...].astype(jnp.float32) + part(tp)
    late_first = list(range(1, blocks)) + [0]
    for b in late_first:
        pooled_spread(b).pass_on()
    if relay:
        for b in late_first:
            pooled_spread(b).finish_near()
        acc[...] += part(2 * (tp // 2) + 1 - tp % 2)
        acc[...] += part((tp + 2) % 4)
        for b in late_first:
            pooled_spread(b).finish()
        acc[...] += part(3 - tp)
    else:
        for b in late_first:
            pooled_spread(b).finish()

        @pl.loop(1, n_tp)
        def _(j):
            acc[...] += part(lax.rem(tp + j, n_tp))

    upf = acc[...].astype(jnp.bfloat16).astype(jnp.float32)
    acc[...] = upf
    gain = norm_gain[:, pl.ds(pl.multiple_of(tp * cols, LANES), cols)]
    plain = (acc[...] * gain).astype(jnp.bfloat16)

    def source(k):
        bits = range(max(1, (chips - 1).bit_length()))
        return sum(((my_chip // 2**b + k // 2**b) % 2) * 2**b for b in bits)

    inner = ((my_chip + 1) // 2) % 2

    def pick_by(i, mid, edge):
        value = 0
        for at, (a, b) in enumerate(zip(mid, edge)):
            value = value + jnp.where(i == at, b + (a - b) * inner, 0)
        return value

    def dispatch(chip, core):
        return remote(
            send.at[chip, core],
            rows.at[my_chip, tp, my_core],
            d_send.at[chip * CORES + core],
            d_recv.at[sp],
            (chip * CORES + core, tp),
        )

    def dispatch_scale(chip, core):
        return remote(
            scale_send.at[chip, core],
            scale_rows.at[my_chip, my_core],
            e_send.at[chip * CORES + core],
            e_recv.at[sp],
            (chip * CORES + core, tp),
        )

    place = lax.broadcasted_iota(jnp.int32, (flat, length), 0).astype(jnp.float32)

    def choose(k):
        chip = source(k)
        here = place + (chip * flat).astype(jnp.float32)
        pick = sum((here == slot[j]).astype(jnp.float32) for j in range(TOPK)).astype(jnp.bfloat16)
        chosen = jnp.dot(pick, plain, preferred_element_type=jnp.float32).astype(jnp.bfloat16)
        send[chip] = chosen.reshape(CORES, cap, cols)
        if k == 0:
            rows[my_chip, tp, my_core] = send[my_chip, my_core]
            dispatch(my_chip, 1 - my_core).start()

    def start_send(k, cores):
        for core in cores:
            dispatch(source(k), core).start()

    def spread_of(buf, ssem, rsem, chip):
        def block(owner, piece):
            return buf.at[chip, owner, piece] if relay else buf.at[chip, owner]

        return Spread(
            n_tp, sp, tp, block, lambda i: ssem.at[chip, i], lambda owner, piece: rsem.at[chip, owner, piece]
        )

    def row_spread(chip):
        return spread_of(rows, f_send, f_recv, chip)

    def act_spread(chip):
        return spread_of(act, a_send, a_recv, chip)

    def start_rows(chip):
        for core in range(CORES):

            @pl.when(chip * CORES + core != sp)
            def _():
                remote(
                    send.at[chip, core],
                    rows.at[chip, tp, core],
                    d_send.at[0],
                    d_recv.at[chip * CORES + core],
                    (chip * CORES + core, tp),
                ).wait_recv()

        row_spread(chip).start()

    first, rest = send_order(chips)
    held = chips == 4

    def send_first(k):
        choose(k)
        if k:
            start_send(k, range(CORES))

    if held:

        @pl.when(inner == 1)
        def _():
            send_first(3)

    for k in first:
        send_first(k)
    squares = jnp.sum(acc[...] * acc[...], axis=1, keepdims=True)
    own = jnp.broadcast_to(squares, (length, LANES)).T[0:8]
    mine[...] = own
    small = [
        remote(mine, sums.at[tp], s_send.at[j - 1], s_recv.at[tp], (sp, lax.rem(tp + j, n_tp)))
        for j in range(1, n_tp)
    ]
    for copy in small:
        copy.start()
    start_rows(my_chip)

    for j in range(1, n_tp):
        owner = lax.rem(tp + n_tp - j, n_tp)
        remote(mine, sums.at[owner], s_send.at[0], s_recv.at[owner], (sp, owner)).wait_recv()
        own = own + sums[owner]
    scale = lax.rsqrt(own[0:1] / (cols * n_tp) + EPS)
    slots_here = lax.broadcasted_iota(jnp.int32, (room, length), 0).astype(jnp.float32)
    for k in first + rest:
        chip = source(k)
        for core in range(CORES):
            here = slots_here + (chip * flat + core * cap).astype(jnp.float32)
            mine_here = sum(jnp.where(here == slot[j], scale, 0.0) for j in range(TOPK))
            column = jnp.sum(mine_here, axis=1, keepdims=True)
            line = jnp.broadcast_to(column, (room, LANES)).T[0:8]
            scale_send[chip, core] = line

            @pl.when(chip * CORES + core == sp)
            def _():
                scale_rows[my_chip, my_core] = scale_send[my_chip, my_core]

            @pl.when(chip * CORES + core != sp)
            def _():
                dispatch_scale(chip, core).start()

    for k in rest:

        @pl.when((inner == 0) | (k != 3))
        def _():
            choose(k)

    def hold(chip):
        @pl.when(inner == 1)
        def _():
            for k in (1, 3):
                for core in range(CORES):
                    dispatch(source(k), core).wait_send()
                    dispatch_scale(source(k), core).wait_send()
            for k in (1, 2, 3):
                for core in range(CORES):
                    pl.semaphore_signal(
                        credit, inc=1, device_id=(source(k) * CORES + core, tp), device_id_type=MESH
                    )
            pl.semaphore_wait(credit, CORES)
            start_send(2, range(CORES))

        @pl.when(inner == 0)
        def _():
            pl.semaphore_wait(credit, 2 * CORES)
            for k in rest:
                start_send(k, range(CORES))

    def give_back(chip, core, at=slice(None)):
        return remote(
            prod.at[chip, core, :, at],
            ret.at[my_chip, my_core, :, at],
            r_send.at[chip * CORES + core],
            r_recv.at[sp],
            (chip * CORES + core, tp),
        )

    tile = min(hidden, 256)
    wide = min(cols, 256)

    def activate(chip):
        for core in range(CORES):

            @pl.when(chip * CORES + core != sp)
            def _():
                remote(
                    scale_send.at[chip, core],
                    scale_rows.at[chip, core],
                    e_send.at[0],
                    e_recv.at[chip * CORES + core],
                    (chip * CORES + core, tp),
                ).wait_recv()

        column = jnp.concatenate(
            [
                jnp.broadcast_to(scale_rows[chip, core, 0:1], (LANES, room)).T[:cap, 0:1]
                for core in range(CORES)
            ],
            axis=0,
        )

        @pl.loop(0, hidden // tile)
        def _(n):
            at = pl.ds(pl.multiple_of(n * tile, tile), tile)
            gate = jnp.zeros((flat, tile), jnp.float32)
            up = jnp.zeros((flat, tile), jnp.float32)
            for t in range(n_tp):
                block = rows[chip, t].reshape(flat, cols)
                deep = pl.ds(t * cols, cols)
                gate += jnp.dot(block, w_gate[deep, at], preferred_element_type=jnp.float32)
                up += jnp.dot(block, w_up[deep, at], preferred_element_type=jnp.float32)
            value = (jax.nn.silu(gate * column) * (up * column)).astype(jnp.bfloat16)
            act[chip, tp, :, :, at] = value.reshape(CORES, cap, tile)

    def produce(chip):
        @pl.loop(0, cols // wide)
        def _(n):
            at = pl.ds(pl.multiple_of(n * wide, wide), wide)
            total = jnp.zeros((flat, wide), jnp.float32)
            for t in range(n_tp):
                block = act[chip, t].reshape(flat, hidden)
                deep = pl.ds(t * hidden, hidden)
                total += jnp.dot(block, w_down[deep, at], preferred_element_type=jnp.float32)
            prod[chip, :, :, at] = total.astype(jnp.bfloat16).reshape(CORES, cap, wide)
            for core in range(CORES):

                @pl.when(chip * CORES + core != sp)
                def _():
                    give_back(chip, core, at).start()

    def finish_rows(chip):
        row_spread(chip).finish_near()
        row_spread(chip).finish()
        activate(chip)

    def finish_act(chip):
        act_spread(chip).finish_near()
        act_spread(chip).finish()
        produce(chip)

        @pl.when(chip == my_chip)
        def _():
            ret[my_chip, my_core] = prod[my_chip, my_core]

    lane = lax.broadcasted_iota(jnp.int32, (length, flat), 1).astype(jnp.float32)

    def combine(chip):
        here = lane + (chip * flat).astype(jnp.float32)
        weight = sum(
            jnp.where(slot_column[j] == here, weight_column[j], 0.0) for j in range(TOPK)
        )
        upper = weight.astype(jnp.bfloat16)
        lower = (weight - upper.astype(jnp.float32)).astype(jnp.bfloat16)
        for core in range(CORES):

            @pl.when(chip * CORES + core != sp)
            def _():
                remote(
                    prod.at[chip, core],
                    ret.at[chip, core],
                    r_send.at[0],
                    r_recv.at[chip * CORES + core],
                    (chip * CORES + core, tp),
                ).wait_recv()

        back = ret[chip].reshape(flat, cols)
        acc[...] += jnp.dot(upper, back, preferred_element_type=jnp.float32) + jnp.dot(
            lower, back, preferred_element_type=jnp.float32
        )

    stages = [
        start_rows,
        lambda chip: row_spread(chip).pass_on(),
        finish_rows,
        lambda chip: act_spread(chip).start(),
        lambda chip: act_spread(chip).pass_on(),
        finish_act,
        combine,
        hold,
    ]
    mid, edge = [
        [STAGES.index(name) * chips + k for name, k in steps] for steps in schedules(chips)
    ]
    for copy in loads[1:]:
        copy.wait()

    @pl.loop(0, len(mid))
    def _(i):
        code = pick_by(i, mid, edge)
        chip = source(code % chips)
        for at, stage in enumerate(stages):

            @pl.when(code // chips == at)
            def _():
                stage(chip)

    out[...] = acc[...]

    @pl.when(sp < n_sp - 1)
    def _():
        for copy in halo_copies(sp + 1):
            copy.wait_send()

    for copy in small:
        copy.wait_send()
    for b in range(blocks):
        pooled_spread(b).sent()
    for copy in (dispatch, dispatch_scale, give_back):
        copy(my_chip, 1 - my_core).wait_send()

    @pl.loop(1, chips)
    def _(k):
        for core in range(CORES):
            give_back(source(k), core).wait_send()

            @pl.when((inner == 0) | (k == 2) | (not held))
            def _():
                for copy in (dispatch, dispatch_scale):
                    copy(source(k), core).wait_send()

    @pl.loop(0, chips)
    def _(chip):
        row_spread(chip).sent()
        act_spread(chip).sent()


def shards(
    residual,
    pool_in,
    docs,
    pool_weight,
    pool_gain,
    out_weight,
    norm_gain,
    routes,
    route_weights,
    w_gate,
    w_up,
    w_down,
):
    length, width = pool_in.shape
    cols = residual.shape[1]
    hidden = w_gate.shape[2]
    n_sp, n_tp = lax.axis_size("sp"), lax.axis_size("tp")
    chips = n_sp // CORES
    cap = length * TOPK * 3 // (2 * n_sp)
    room = -(-cap // LANES) * LANES
    blocks = length // LANES
    pieces = 2 if n_tp == 4 else 1
    fan = 6 if n_tp == 4 else n_tp
    dma = pltpu.SemaphoreType.DMA
    vmem = pl.BlockSpec(memory_space=pltpu.VMEM)
    hbm = pl.BlockSpec(memory_space=pl.ANY)
    half = jnp.bfloat16
    return pl.pallas_call(
        functools.partial(layer_kernel, n_sp, n_tp),
        out_shape=pltpu.VMEM((length, cols), jnp.float32),
        in_specs=[hbm] * 12,
        out_specs=vmem,
        scratch_shapes=[
            pltpu.VMEM((length, cols), half),
            pltpu.VMEM((length, width), half),
            pltpu.VMEM((1, length), jnp.int32),
            pltpu.VMEM(pool_weight.shape, half),
            pltpu.VMEM((1, width), jnp.float32),
            pltpu.VMEM((1, *norm_gain.shape), jnp.float32),
            pltpu.VMEM((TOPK, length), jnp.int32),
            pltpu.VMEM((TOPK, length), jnp.float32),
            pltpu.VMEM((LANES + length, width), half),
            pltpu.VMEM((TAIL, width), half),
            pltpu.VMEM((1, LANES), jnp.int32),
            pltpu.VMEM((n_tp, length, width), half),
            pltpu.VMEM((length, cols), jnp.float32),
            pltpu.VMEM((8, length), jnp.float32),
            pltpu.VMEM((n_tp, 8, length), jnp.float32),
            pltpu.VMEM((chips, CORES, cap, cols), half),
            pltpu.VMEM((chips, n_tp, CORES, cap, cols), half),
            pltpu.VMEM((chips, n_tp, CORES, cap, hidden), half),
            pltpu.VMEM((chips, CORES, cap, cols), half),
            pltpu.VMEM((chips, CORES, cap, cols), half),
            pltpu.VMEM((chips, CORES, 8, room), jnp.float32),
            pltpu.VMEM((chips, CORES, 8, room), jnp.float32),
            pltpu.VMEM(out_weight.shape, half),
            pltpu.VMEM(w_gate.shape[1:], half),
            pltpu.VMEM(w_up.shape[1:], half),
            pltpu.VMEM(w_down.shape[1:], half),
            dma((8,)),
            dma((4,)),
            dma((2,)),
            dma((2,)),
            dma((blocks, fan)),
            dma((blocks, n_tp, pieces)),
            dma((n_tp,)),
            dma((n_tp,)),
            dma((n_sp,)),
            dma((n_sp,)),
            dma((chips, fan)),
            dma((chips, n_tp, pieces)),
            dma((chips, fan)),
            dma((chips, n_tp, pieces)),
            dma((n_sp,)),
            dma((n_sp,)),
            dma((n_sp,)),
            dma((n_sp,)),
            pltpu.SemaphoreType.REGULAR,
        ],
        compiler_params=pltpu.CompilerParams(
            collective_id=0, has_side_effects=True, vmem_limit_bytes=VMEM_LIMIT
        ),
    )(
        residual,
        pool_in,
        docs.reshape(1, length),
        pool_weight,
        pool_gain.reshape(1, width),
        norm_gain.reshape(1, -1),
        routes.T,
        route_weights.T,
        out_weight,
        w_gate[0],
        w_up[0],
        w_down[0],
    ).astype(half)


def solution(mesh):
    placed = (
        P("sp", "tp"),
        P("sp", "tp"),
        P("sp"),
        P("tp", None, None),
        P("tp"),
        P(None, "tp"),
        P(),
        P("sp", None),
        P("sp", None),
        P("sp", None, "tp"),
        P("sp", None, "tp"),
        P("sp", None, "tp"),
    )
    return jax.shard_map(
        shards, mesh=mesh, in_specs=placed, out_specs=P("sp", "tp"), check_vma=False
    )
```

```python
import functools

import jax
import jax.numpy as jnp
from jax import lax
from jax.experimental import pallas as pl
from jax.experimental.pallas import tpu as pltpu
from jax.sharding import PartitionSpec as P

GD = 128
TOPK = 2
EPS = 1e-06
MESH = pl.DeviceIdType.MESH
CORES = 2
LANES = 128
TAIL = 16
VMEM_LIMIT = 62 * 1024 * 1024


def remote(src, dst, send_sem, recv_sem, device):
    return pltpu.make_async_remote_copy(
        src_ref=src,
        dst_ref=dst,
        send_sem=send_sem,
        recv_sem=recv_sem,
        device_id=device,
        device_id_type=MESH,
    )


class Spread:
    def __init__(self, n_tp, sp, tp, block, blocks, send_sem, recv_sem):
        self.n_tp, self.sp, self.tp = n_tp, sp, tp
        self.block, self.blocks, self.send_sem, self.recv_sem = block, blocks, send_sem, recv_sem
        self.relay = n_tp == 4
        self.across = 2 * (tp // 2) + 1 - tp % 2
        self.along = (tp + 2) % 4
        self.other = self.across if self.relay else lax.rem(tp + 1, n_tp)

    def copy(self, owner, piece, group, peer):
        ref = self.block(owner, piece)
        return remote(ref, ref, self.send_sem, self.recv_sem(group), (self.sp, peer))

    def direct(self):
        if self.relay:
            return [
                self.copy(self.tp, 0, 0, self.across),
                self.copy(self.tp, 1, 0, self.along),
                self.copy(self.tp, 1, 1, self.across),
                self.copy(self.tp, 0, 1, self.along),
            ]
        return [self.copy(self.tp, 0, 0, lax.rem(self.tp + j, self.n_tp)) for j in range(1, self.n_tp)]

    def start(self):
        for copy in self.direct():
            copy.start()

    def all_of(self, group, count):
        ref = self.blocks(count)
        return remote(ref, ref, self.send_sem, self.recv_sem(group), (self.sp, self.other))

    def pass_on(self):
        if self.relay:
            self.all_of(0, 1).wait_recv()
            self.copy(self.across, 0, 2, self.along).start()
            self.copy(self.along, 1, 2, self.across).start()

    def finish_near(self):
        if self.relay:
            self.all_of(1, 1).wait_recv()

    def finish(self):
        if self.relay:
            self.all_of(2, 1).wait_recv()
        else:
            self.all_of(0, self.n_tp - 1).wait_recv()

    def sent(self):
        self.all_of(0, self.n_tp - 1).wait_send()


STAGES = ["D", "RD", "CD", "A", "RA", "CA", "C", "Z", "E", "W"]
MID = (
    "RD0 Z0 D3 RD3",
    "D1 CD3 A3 RA3",
    "D2 CD0 CA3 RD2",
    "RD1 CD2 A2 CD1",
    "RA2 A1 CA2 RA1",
    "A0 C3 CA1 RA0",
    "C1 W0 CA0 C0",
    "E2",
)
EDGE = (
    "RD0 Z0 D1 CD0",
    "RD1 D3 RD3 D2",
    "CD3 CD1 A3 RA3",
    "RD2 A1 CA3 CD2",
    "RA1 A2 CA1 RA2",
    "A0 CA2 RA0 C3",
    "W0 CA0 C2 C0",
    "E1",
)


def schedules(chips):
    if chips == 4:
        return [[(step[:-1], int(step[-1])) for step in " ".join(plan).split()] for plan in (MID, EDGE)]
    steps = [("RD", 0)]
    for k in range(1, chips):
        steps += [("D", k), ("RD", k), ("CD", k - 1), ("A", k - 1), ("RA", k - 1), ("CA", k - 1)]
    last = chips - 1
    steps += [("CD", last), ("A", last), ("RA", last), ("CA", last)]
    steps += [("C", k) for k in range(chips - 1)] + [("W", 0), ("E", last)]
    return steps, steps


def send_order(chips):
    return ([0, 1], [3, 2]) if chips == 4 else (list(range(chips)), [])


def layer_kernel(
    n_sp,
    n_tp,
    residual_hbm,
    pool_in_hbm,
    docs_hbm,
    pool_weight_hbm,
    pool_gain_hbm,
    norm_gain_hbm,
    routes_hbm,
    route_weights_hbm,
    wout_hbm,
    gate_hbm,
    up_hbm,
    down_hbm,
    out,
    residual,
    pool_in,
    docs,
    pool_weight,
    pool_gain,
    norm_gain,
    routes,
    route_weights,
    ext,
    halo,
    halo_docs,
    gathered,
    acc,
    mine,
    sums,
    send,
    rows,
    act,
    prod,
    ret,
    scale_send,
    scale_rows,
    partial,
    wout,
    w_gate,
    w_up,
    w_down,
    in_sem,
    load_sem,
    h_send,
    h_recv,
    p_send,
    p_recv,
    s_send,
    s_recv,
    d_send,
    d_recv,
    f_send,
    f_recv,
    a_send,
    a_recv,
    r_send,
    r_recv,
    e_send,
    e_recv,
    credit,
):
    sp, tp = lax.axis_index("sp"), lax.axis_index("tp")
    chips = n_sp // CORES
    my_chip, my_core = sp // CORES, sp % CORES
    length, width = pool_in.shape
    cols = residual.shape[1]
    cap = send.shape[2]
    hidden = act.shape[4]
    flat = CORES * cap
    experts = n_sp
    relay = n_tp == 4
    room = -(-cap // LANES) * LANES

    loads = [
        pltpu.make_async_copy(wout_hbm, wout, load_sem.at[0]),
        pltpu.make_async_copy(gate_hbm, w_gate, load_sem.at[1]),
        pltpu.make_async_copy(up_hbm, w_up, load_sem.at[2]),
        pltpu.make_async_copy(down_hbm, w_down, load_sem.at[3]),
    ]
    barrier = pltpu.get_barrier_semaphore()
    peers = [(lax.rem(sp + j, n_sp), tp) for j in range(1, n_sp)]
    peers += [(sp, lax.rem(tp + j, n_tp)) for j in range(1, n_tp)]
    for device in peers:
        pl.semaphore_signal(barrier, inc=1, device_id=device, device_id_type=MESH)
    inputs = [
        pltpu.make_async_copy(src, dst, in_sem.at[at])
        for at, (src, dst) in enumerate(
            (
                (routes_hbm, routes),
                (route_weights_hbm, route_weights),
                (docs_hbm, docs),
                (pool_in_hbm, pool_in),
                (pool_weight_hbm, pool_weight),
                (pool_gain_hbm, pool_gain),
                (norm_gain_hbm, norm_gain),
                (residual_hbm, residual),
            )
        )
    ]
    for copy in inputs:
        copy.start()
    for copy in inputs[2:6]:
        copy.wait()

    doc_row = docs[...].astype(jnp.float32)
    doc_column = jnp.broadcast_to(doc_row, (LANES, length)).T[:, 0:1]
    ext[0 : LANES - TAIL, :] = jnp.zeros((LANES - TAIL, width), jnp.bfloat16)
    ext[LANES:, :] = pool_in[...]

    blocks = length // LANES
    away = (
        LANES
        + lax.broadcasted_iota(jnp.int32, (LANES, 2 * LANES), 0)
        - lax.broadcasted_iota(jnp.int32, (LANES, 2 * LANES), 1)
    )
    half = LANES // 2

    def pooled_spread(b):
        def block(owner, piece):
            if relay:
                return gathered.at[owner, pl.ds(b * LANES + piece * half, half), :]
            return gathered.at[owner, pl.ds(b * LANES, LANES), :]

        def several(count):
            return gathered.at[pl.ds(0, count), pl.ds(b * LANES, LANES), :]

        return Spread(n_tp, sp, tp, block, several, p_send.at[b], lambda group: p_recv.at[b, group])

    def pool(b, prior):
        low = b * LANES
        near = (doc_column[low : low + LANES, :] == prior) & (away >= 0)
        groups = width // GD
        for g in range(groups):
            if groups % 4 == 0:
                span = 2 << (g % 4)
            else:
                span = lax.shift_left(jnp.int32(2), (tp * groups + g) % 4)
            weight = (near & (away < span)).astype(jnp.float32)
            at = slice(g * GD, (g + 1) * GD)
            count = jnp.sum(weight, axis=1, keepdims=True)
            total = jnp.dot(
                weight.astype(jnp.bfloat16), ext[low : low + 2 * LANES, at], preferred_element_type=jnp.float32
            )
            own = ext[low + LANES : low + 2 * LANES, at].astype(jnp.float32)
            diff = (total / count - own).astype(jnp.bfloat16)
            mixed = jnp.dot(diff, pool_weight[g], preferred_element_type=jnp.float32)
            gathered[tp, low : low + LANES, at] = (mixed * pool_gain[:, at]).astype(jnp.bfloat16)

    for b in range(1, blocks):
        pool(b, doc_row[:, (b - 1) * LANES : (b + 1) * LANES])

    pl.semaphore_wait(barrier, len(peers))

    def halo_copies(to):
        return [
            remote(docs.at[:, length - LANES :], halo_docs, h_send.at[0], h_recv.at[0], (to, tp)),
            remote(pool_in.at[length - TAIL :, :], halo, h_send.at[1], h_recv.at[1], (to, tp)),
        ]

    @pl.when(sp < n_sp - 1)
    def _():
        for copy in halo_copies(sp + 1):
            copy.start()

    for b in range(1, blocks):
        pooled_spread(b).start()
    for copy in inputs[:2] + inputs[6:]:
        copy.wait()
    for copy in loads:
        copy.start()

    high = max(16, experts)
    route = [routes[k : k + 1, :] for k in range(TOPK)]
    expert = lax.broadcasted_iota(jnp.int32, (high, length), 0)
    used = sum((expert == route[k]).astype(jnp.float32) for k in range(TOPK))
    before = lax.broadcasted_iota(jnp.int32, (length, length), 0) < lax.broadcasted_iota(
        jnp.int32, (length, length), 1
    )
    taken = jnp.dot(
        used.astype(jnp.bfloat16), before.astype(jnp.bfloat16), preferred_element_type=jnp.float32
    )
    slot = []
    for k in range(TOPK):
        rank = jnp.sum(jnp.where(expert == route[k], taken, 0.0), axis=0, keepdims=True)
        slot.append(route[k].astype(jnp.float32) * cap + rank)
    line = lax.broadcasted_iota(jnp.int32, (LANES, length), 0)
    table = jnp.zeros((LANES, length), jnp.float32)
    for k in range(TOPK):
        table = jnp.where(line == k, slot[k], table)
    columns = table.T
    slot_column = [columns[:, k : 1 + k] for k in range(TOPK)]

    @pl.when(sp == 0)
    def _():
        halo[...] = jnp.zeros_like(halo)
        halo_docs[...] = jnp.full_like(halo_docs, -1)

    @pl.when(sp > 0)
    def _():
        for copy in halo_copies(sp - 1):
            copy.wait_recv()

    ext[LANES - TAIL : LANES, :] = halo[...]
    first_docs = halo_docs[...].astype(jnp.float32)
    pool(0, jnp.concatenate([first_docs, doc_row[:, :LANES]], axis=1))
    pooled_spread(0).start()

    def part(owner):
        deep = pl.ds(pl.multiple_of(owner * width, width), width)
        return jnp.dot(gathered[owner], wout[deep, :], preferred_element_type=jnp.float32)

    loads[0].wait()
    acc[...] = residual[...].astype(jnp.float32) + part(tp)
    late_first = list(range(1, blocks)) + [0]
    for b in late_first:
        pooled_spread(b).pass_on()
    if relay:
        for b in late_first:
            pooled_spread(b).finish_near()
        acc[...] += part(2 * (tp // 2) + 1 - tp % 2)
        acc[...] += part((tp + 2) % 4)
        for b in late_first:
            pooled_spread(b).finish()
        acc[...] += part(3 - tp)
    else:
        for b in late_first:
            pooled_spread(b).finish()

        @pl.loop(1, n_tp)
        def _(j):
            acc[...] += part(lax.rem(tp + j, n_tp))

    upf = acc[...].astype(jnp.bfloat16).astype(jnp.float32)
    acc[...] = upf
    gain = norm_gain[:, pl.ds(pl.multiple_of(tp * cols, LANES), cols)]
    plain = (acc[...] * gain).astype(jnp.bfloat16)

    def source(k):
        bits = range(max(1, (chips - 1).bit_length()))
        return sum(((my_chip // 2**b + k // 2**b) % 2) * 2**b for b in bits)

    inner = ((my_chip + 1) // 2) % 2

    def pick_by(i, mid, edge):
        value = 0
        for at, (a, b) in enumerate(zip(mid, edge)):
            value = value + jnp.where(i == at, b + (a - b) * inner, 0)
        return value

    held = chips == 4

    def group(k):
        return 0 if k == 0 else 2 if held and k == 2 else 1

    def dispatch(k, core):
        return remote(
            send.at[source(k), core],
            rows.at[my_chip, tp, my_core],
            d_send.at[group(k)],
            d_recv.at[my_chip],
            (source(k) * CORES + core, tp),
        )

    def dispatch_scale(k, core):
        return remote(
            scale_send.at[source(k), core],
            scale_rows.at[my_chip, my_core],
            e_send.at[group(k)],
            e_recv.at[my_chip],
            (source(k) * CORES + core, tp),
        )

    partner = (my_chip * CORES + 1 - my_core, tp)

    def dispatched(at):
        few = [1, 2] if held else [1, chips - 1]
        for buf, sem in ((send, d_send), (scale_send, e_send)):
            ref = buf.at[0, 0] if at == 0 else buf.at[0] if at == 2 else buf.at[pl.ds(0, few[1])]
            remote(ref, ref, sem.at[at], d_recv.at[0], partner).wait_send()

    def arrived(chip, sem, both, one):
        @pl.when(chip != my_chip)
        def _():
            remote(both, both, sem.at[chip], sem.at[chip], partner).wait_recv()

        @pl.when(chip == my_chip)
        def _():
            remote(one, one, sem.at[chip], sem.at[chip], partner).wait_recv()

    place = lax.broadcasted_iota(jnp.int32, (flat, length), 0).astype(jnp.float32)

    def choose(k):
        chip = source(k)
        here = place + (chip * flat).astype(jnp.float32)
        pick = sum((here == slot[j]).astype(jnp.float32) for j in range(TOPK)).astype(jnp.bfloat16)
        chosen = jnp.dot(pick, plain, preferred_element_type=jnp.float32).astype(jnp.bfloat16)
        send[chip] = chosen.reshape(CORES, cap, cols)
        if k == 0:
            rows[my_chip, tp, my_core] = send[my_chip, my_core]
            dispatch(0, 1 - my_core).start()

    def start_send(k, cores):
        for core in cores:
            dispatch(k, core).start()

    def spread_of(buf, ssem, rsem, chip):
        def block(owner, piece):
            return buf.at[chip, owner, piece] if relay else buf.at[chip, owner]

        def several(count):
            return buf.at[chip, pl.ds(0, count)]

        return Spread(n_tp, sp, tp, block, several, ssem.at[chip], lambda group: rsem.at[chip, group])

    def row_spread(chip):
        return spread_of(rows, f_send, f_recv, chip)

    def act_spread(chip):
        return spread_of(act, a_send, a_recv, chip)

    def await_rows(chip):
        arrived(chip, d_recv, rows.at[chip, tp], rows.at[chip, tp, 0])

    def start_rows(chip):
        await_rows(chip)
        row_spread(chip).start()

    first, rest = send_order(chips)

    def send_first(k):
        choose(k)
        if k:
            start_send(k, range(CORES))

    if held:

        @pl.when(inner == 1)
        def _():
            send_first(3)

    def start_own(core):
        @pl.when(my_core == core)
        def _():
            if core == 1 and relay:
                await_rows(my_chip)
                for copy in row_spread(my_chip).direct()[0::3]:
                    copy.start()
            else:
                start_rows(my_chip)

    send_first(0)
    squares = jnp.sum(acc[...] * acc[...], axis=1, keepdims=True)
    own = jnp.broadcast_to(squares, (length, LANES)).T[0:8]
    mine[...] = own
    small = [
        remote(mine, sums.at[tp], s_send.at[0], s_recv.at[0], (sp, lax.rem(tp + j, n_tp)))
        for j in range(1, n_tp)
    ]
    for copy in small:
        copy.start()

    def all_sums():
        ref = sums.at[pl.ds(0, n_tp - 1)]
        return remote(ref, ref, s_send.at[0], s_recv.at[0], (sp, lax.rem(tp + 1, n_tp)))

    start_own(0)
    if relay:

        @pl.when(my_core == 1)
        def _():
            for copy in row_spread(my_chip).direct()[1:3]:
                copy.start()

    for k in first[1:]:
        send_first(k)
    start_own(1)

    all_sums().wait_recv()
    for j in range(1, n_tp):
        own = own + sums[lax.rem(tp + n_tp - j, n_tp)]
    scale = lax.rsqrt(own[0:1] / (cols * n_tp) + EPS)
    slots_here = lax.broadcasted_iota(jnp.int32, (room, length), 0).astype(jnp.float32)
    for k in first + rest:
        chip = source(k)
        for core in range(CORES):
            here = slots_here + (chip * flat + core * cap).astype(jnp.float32)
            mine_here = sum(jnp.where(here == slot[j], scale, 0.0) for j in range(TOPK))
            weigh = sum(
                jnp.where(here == slot[j], route_weights[j : j + 1, :], 0.0) for j in range(TOPK)
            )
            pair = jnp.where(
                lax.broadcasted_iota(jnp.int32, (room, LANES), 1) == 0,
                jnp.sum(mine_here, axis=1, keepdims=True),
                jnp.sum(weigh, axis=1, keepdims=True),
            )
            scale_send[chip, core] = pair.T[0:8]

            @pl.when(chip * CORES + core == sp)
            def _():
                scale_rows[my_chip, my_core] = scale_send[my_chip, my_core]

            @pl.when(chip * CORES + core != sp)
            def _():
                dispatch_scale(k, core).start()

    for k in rest:

        @pl.when((inner == 0) | (k != 3))
        def _():
            choose(k)

    def hold(chip):
        @pl.when(inner == 1)
        def _():
            dispatched(1)
            for k in (1, 2, 3):
                for core in range(CORES):
                    pl.semaphore_signal(
                        credit, inc=1, device_id=(source(k) * CORES + core, tp), device_id_type=MESH
                    )
            pl.semaphore_wait(credit, CORES)
            start_send(2, range(CORES))

        @pl.when(inner == 0)
        def _():
            pl.semaphore_wait(credit, 2 * CORES)
            for k in rest:
                start_send(k, range(CORES))

    def give_back(chip, core, at=slice(None)):
        return remote(
            prod.at[chip, core, :, at],
            ret.at[my_chip, my_core, :, at],
            r_send.at[chip],
            r_recv.at[my_chip],
            (chip * CORES + core, tp),
        )

    tile = min(hidden, 256)
    wide = min(cols, 256)

    def slot_numbers(chip, which):
        return jnp.concatenate(
            [
                jnp.broadcast_to(scale_rows[chip, core, which : which + 1], (LANES, room)).T[:cap, 0:1]
                for core in range(CORES)
            ],
            axis=0,
        )

    def activate(chip):
        arrived(chip, e_recv, scale_rows.at[chip], scale_rows.at[chip, 0])
        column = slot_numbers(chip, 0)

        @pl.loop(0, hidden // tile)
        def _(n):
            at = pl.ds(pl.multiple_of(n * tile, tile), tile)
            gate = jnp.zeros((flat, tile), jnp.float32)
            up = jnp.zeros((flat, tile), jnp.float32)
            for t in range(n_tp):
                block = rows[chip, t].reshape(flat, cols)
                deep = pl.ds(t * cols, cols)
                gate += jnp.dot(block, w_gate[deep, at], preferred_element_type=jnp.float32)
                up += jnp.dot(block, w_up[deep, at], preferred_element_type=jnp.float32)
            value = (jax.nn.silu(gate * column) * (up * column)).astype(jnp.bfloat16)
            act[chip, tp, :, :, at] = value.reshape(CORES, cap, tile)

    def products(chip, owners, at):
        total = jnp.zeros((flat, wide), jnp.float32)
        for t in owners:
            block = act[chip, t].reshape(flat, hidden)
            deep = pl.ds(pl.multiple_of(t * hidden, hidden), hidden)
            total += jnp.dot(block, w_down[deep, at], preferred_element_type=jnp.float32)
        return total

    if relay:
        near, far = [tp, 2 * (tp // 2) + 1 - tp % 2, (tp + 2) % 4], [3 - tp]
    else:
        near, far = [tp], [lax.rem(tp + j, n_tp) for j in range(1, n_tp)]

    def tiles(n):
        return pl.ds(pl.multiple_of(n * wide, wide), wide)

    def produce_near(chip):
        @pl.loop(0, cols // wide)
        def _(n):
            partial[:, tiles(n)] = products(chip, near, tiles(n))

    def produce(chip):
        weigh = slot_numbers(chip, 1)

        @pl.loop(0, cols // wide)
        def _(n):
            at = tiles(n)
            total = (partial[:, at] + products(chip, far, at)) * weigh
            prod[chip, :, :, at] = total.astype(jnp.bfloat16).reshape(CORES, cap, wide)
            for core in range(CORES):

                @pl.when(chip * CORES + core != sp)
                def _():
                    give_back(chip, core, at).start()

    def finish_rows(chip):
        row_spread(chip).finish_near()
        row_spread(chip).finish()
        activate(chip)

    def finish_act(chip):
        act_spread(chip).finish_near()
        produce_near(chip)
        act_spread(chip).finish()
        produce(chip)

        @pl.when(chip == my_chip)
        def _():
            ret[my_chip, my_core] = prod[my_chip, my_core]

    lane = lax.broadcasted_iota(jnp.int32, (length, flat), 1).astype(jnp.float32)

    def returned(chip):
        here = lane + (chip * flat).astype(jnp.float32)
        pick = sum((slot_column[j] == here).astype(jnp.float32) for j in range(TOPK)).astype(jnp.bfloat16)
        arrived(chip, r_recv, ret.at[chip], ret.at[chip, 0])
        return acc[...] + jnp.dot(pick, ret[chip].reshape(flat, cols), preferred_element_type=jnp.float32)

    def combine(chip):
        acc[...] = returned(chip)

    def combine_last(chip):
        out[...] = returned(chip)

    def settle(_chip):
        @pl.when(sp < n_sp - 1)
        def _():
            for copy in halo_copies(sp + 1):
                copy.wait_send()

        all_sums().wait_send()
        for b in range(blocks):
            pooled_spread(b).sent()
        dispatched(0)
        if held:

            @pl.when(inner == 0)
            def _():
                dispatched(1)

            dispatched(2)
        else:
            dispatched(1)

        @pl.loop(0, chips)
        def _(chip):
            row_spread(chip).sent()

    stages = [
        start_rows,
        lambda chip: row_spread(chip).pass_on(),
        finish_rows,
        lambda chip: act_spread(chip).start(),
        lambda chip: act_spread(chip).pass_on(),
        finish_act,
        combine,
        hold,
        combine_last,
        settle,
    ]
    mid, edge = [
        [STAGES.index(name) * chips + k for name, k in steps] for steps in schedules(chips)
    ]
    for copy in loads[1:]:
        copy.wait()

    @pl.loop(0, len(mid))
    def _(i):
        code = pick_by(i, mid, edge)
        chip = source(code % chips)
        for at, stage in enumerate(stages):

            @pl.when(code // chips == at)
            def _():
                stage(chip)

    @pl.loop(0, chips)
    def _(chip):
        act_spread(chip).sent()

        @pl.when(chip != my_chip)
        def _():
            remote(prod.at[chip], prod.at[chip], r_send.at[chip], r_recv.at[0], partner).wait_send()

        @pl.when(chip == my_chip)
        def _():
            remote(prod.at[chip, 0], prod.at[chip, 0], r_send.at[chip], r_recv.at[0], partner).wait_send()


def shards(
    residual,
    pool_in,
    docs,
    pool_weight,
    pool_gain,
    out_weight,
    norm_gain,
    routes,
    route_weights,
    w_gate,
    w_up,
    w_down,
):
    length, width = pool_in.shape
    cols = residual.shape[1]
    hidden = w_gate.shape[2]
    n_sp, n_tp = lax.axis_size("sp"), lax.axis_size("tp")
    chips = n_sp // CORES
    cap = length * TOPK * 3 // (2 * n_sp)
    room = -(-cap // LANES) * LANES
    blocks = length // LANES
    groups = 3 if n_tp == 4 else 1
    dma = pltpu.SemaphoreType.DMA
    vmem = pl.BlockSpec(memory_space=pltpu.VMEM)
    hbm = pl.BlockSpec(memory_space=pl.ANY)
    half = jnp.bfloat16
    return pl.pallas_call(
        functools.partial(layer_kernel, n_sp, n_tp),
        out_shape=pltpu.VMEM((length, cols), jnp.float32),
        in_specs=[hbm] * 12,
        out_specs=vmem,
        scratch_shapes=[
            pltpu.VMEM((length, cols), half),
            pltpu.VMEM((length, width), half),
            pltpu.VMEM((1, length), jnp.int32),
            pltpu.VMEM(pool_weight.shape, half),
            pltpu.VMEM((1, width), jnp.float32),
            pltpu.VMEM((1, *norm_gain.shape), jnp.float32),
            pltpu.VMEM((TOPK, length), jnp.int32),
            pltpu.VMEM((TOPK, length), jnp.float32),
            pltpu.VMEM((LANES + length, width), half),
            pltpu.VMEM((TAIL, width), half),
            pltpu.VMEM((1, LANES), jnp.int32),
            pltpu.VMEM((n_tp, length, width), half),
            pltpu.VMEM((length, cols), jnp.float32),
            pltpu.VMEM((8, length), jnp.float32),
            pltpu.VMEM((n_tp, 8, length), jnp.float32),
            pltpu.VMEM((chips, CORES, cap, cols), half),
            pltpu.VMEM((chips, n_tp, CORES, cap, cols), half),
            pltpu.VMEM((chips, n_tp, CORES, cap, hidden), half),
            pltpu.VMEM((chips, CORES, cap, cols), half),
            pltpu.VMEM((chips, CORES, cap, cols), half),
            pltpu.VMEM((chips, CORES, 8, room), jnp.float32),
            pltpu.VMEM((chips, CORES, 8, room), jnp.float32),
            pltpu.VMEM((CORES * cap, cols), jnp.float32),
            pltpu.VMEM(out_weight.shape, half),
            pltpu.VMEM(w_gate.shape[1:], half),
            pltpu.VMEM(w_up.shape[1:], half),
            pltpu.VMEM(w_down.shape[1:], half),
            dma((8,)),
            dma((4,)),
            dma((2,)),
            dma((2,)),
            dma((blocks,)),
            dma((blocks, groups)),
            dma((1,)),
            dma((1,)),
            dma((3,)),
            dma((chips,)),
            dma((chips,)),
            dma((chips, groups)),
            dma((chips,)),
            dma((chips, groups)),
            dma((chips,)),
            dma((chips,)),
            dma((3,)),
            dma((chips,)),
            pltpu.SemaphoreType.REGULAR,
        ],
        compiler_params=pltpu.CompilerParams(
            collective_id=0, has_side_effects=True, vmem_limit_bytes=VMEM_LIMIT
        ),
    )(
        residual,
        pool_in,
        docs.reshape(1, length),
        pool_weight,
        pool_gain.reshape(1, width),
        norm_gain.reshape(1, -1),
        routes.T,
        route_weights.T,
        out_weight,
        w_gate[0],
        w_up[0],
        w_down[0],
    ).astype(half)


def solution(mesh):
    placed = (
        P("sp", "tp"),
        P("sp", "tp"),
        P("sp"),
        P("tp", None, None),
        P("tp"),
        P(None, "tp"),
        P(),
        P("sp", None),
        P("sp", None),
        P("sp", None, "tp"),
        P("sp", None, "tp"),
        P("sp", None, "tp"),
    )
    return jax.shard_map(
        shards, mesh=mesh, in_specs=placed, out_specs=P("sp", "tp"), check_vma=False
    )
```

```python
import functools

import jax
import jax.numpy as jnp
from jax import lax
from jax.experimental import pallas as pl
from jax.experimental.pallas import tpu as pltpu
from jax.sharding import PartitionSpec as P

GD = 128
TOPK = 2
EPS = 1e-06
MESH = pl.DeviceIdType.MESH
CORES = 2
LANES = 128
TAIL = 16
VMEM_LIMIT = 62 * 1024 * 1024


def remote(src, dst, send_sem, recv_sem, device):
    return pltpu.make_async_remote_copy(
        src_ref=src,
        dst_ref=dst,
        send_sem=send_sem,
        recv_sem=recv_sem,
        device_id=device,
        device_id_type=MESH,
    )


class Spread:
    def __init__(self, n_tp, sp, tp, block, blocks, send_sem, recv_sem):
        self.n_tp, self.sp, self.tp = n_tp, sp, tp
        self.block, self.blocks, self.send_sem, self.recv_sem = block, blocks, send_sem, recv_sem
        self.relay = n_tp == 4
        self.across = 2 * (tp // 2) + 1 - tp % 2
        self.along = (tp + 2) % 4
        self.other = self.across if self.relay else lax.rem(tp + 1, n_tp)

    def copy(self, owner, piece, group, peer):
        ref = self.block(owner, piece)
        return remote(ref, ref, self.send_sem, self.recv_sem(group), (self.sp, peer))

    def direct(self):
        if self.relay:
            return [
                self.copy(self.tp, 0, 0, self.across),
                self.copy(self.tp, 1, 0, self.along),
                self.copy(self.tp, 1, 1, self.across),
                self.copy(self.tp, 0, 1, self.along),
            ]
        return [self.copy(self.tp, 0, 0, lax.rem(self.tp + j, self.n_tp)) for j in range(1, self.n_tp)]

    def start(self):
        for copy in self.direct():
            copy.start()

    def all_of(self, group, count):
        ref = self.blocks(count)
        return remote(ref, ref, self.send_sem, self.recv_sem(group), (self.sp, self.other))

    def pass_on(self):
        if self.relay:
            self.all_of(0, 1).wait_recv()
            self.copy(self.across, 0, 2, self.along).start()
            self.copy(self.along, 1, 2, self.across).start()

    def finish_near(self):
        if self.relay:
            self.all_of(1, 1).wait_recv()

    def finish(self):
        if self.relay:
            self.all_of(2, 1).wait_recv()
        else:
            self.all_of(0, self.n_tp - 1).wait_recv()

    def sent(self):
        self.all_of(0, self.n_tp - 1).wait_send()


STAGES = ["D", "RD", "CD", "A", "RA", "CA", "C", "Z", "E", "W"]
MID = (
    "RD0 Z0 D3 RD3",
    "D1 CD3 A3 RA3",
    "D2 CD0 CA3 RD2",
    "RD1 CD2 A2 RA2",
    "CD1 A1 CA2 RA1",
    "A0 CA1 C3 RA0",
    "C1 W0 CA0 C0",
    "E2",
)
EDGE = (
    "RD0 Z0 D1 CD0",
    "RD1 D3 RD3 D2",
    "CD3 CD1 A3 RA3",
    "RD2 A1 CA3 CD2",
    "RA1 A2 CA1 RA2",
    "A0 CA2 RA0 C3",
    "W0 CA0 C2 C0",
    "E1",
)


def schedules(chips):
    if chips == 4:
        return [[(step[:-1], int(step[-1])) for step in " ".join(plan).split()] for plan in (MID, EDGE)]
    steps = [("RD", 0)]
    for k in range(1, chips):
        steps += [("D", k), ("RD", k), ("CD", k - 1), ("A", k - 1), ("RA", k - 1), ("CA", k - 1)]
    last = chips - 1
    steps += [("CD", last), ("A", last), ("RA", last), ("CA", last)]
    steps += [("C", k) for k in range(chips - 1)] + [("W", 0), ("E", last)]
    return steps, steps


def send_order(chips):
    return ([0, 1], [3, 2]) if chips == 4 else (list(range(chips)), [])


def layer_kernel(
    n_sp,
    n_tp,
    residual_hbm,
    pool_in_hbm,
    docs_hbm,
    pool_weight_hbm,
    pool_gain_hbm,
    norm_gain_hbm,
    routes_hbm,
    route_weights_hbm,
    wout_hbm,
    gate_hbm,
    up_hbm,
    down_hbm,
    out,
    residual,
    pool_in,
    docs,
    pool_weight,
    pool_gain,
    norm_gain,
    routes,
    route_weights,
    ext,
    halo,
    halo_docs,
    gathered,
    acc,
    mine,
    sums,
    send,
    rows,
    act,
    prod,
    ret,
    scale_send,
    scale_rows,
    partial,
    wout,
    w_gate,
    w_up,
    w_down,
    in_sem,
    load_sem,
    h_send,
    h_recv,
    p_send,
    p_recv,
    s_send,
    s_recv,
    d_send,
    d_recv,
    f_send,
    f_recv,
    a_send,
    a_recv,
    r_send,
    r_recv,
    e_send,
    e_recv,
    credit,
):
    sp, tp = lax.axis_index("sp"), lax.axis_index("tp")
    chips = n_sp // CORES
    my_chip, my_core = sp // CORES, sp % CORES
    length, width = pool_in.shape
    cols = residual.shape[1]
    cap = send.shape[2]
    hidden = act.shape[4]
    flat = CORES * cap
    experts = n_sp
    relay = n_tp == 4
    room = -(-cap // LANES) * LANES

    loads = [
        pltpu.make_async_copy(wout_hbm, wout, load_sem.at[0]),
        pltpu.make_async_copy(gate_hbm, w_gate, load_sem.at[1]),
        pltpu.make_async_copy(up_hbm, w_up, load_sem.at[2]),
        pltpu.make_async_copy(down_hbm, w_down, load_sem.at[3]),
    ]
    barrier = pltpu.get_barrier_semaphore()
    peers = [(lax.rem(sp + j, n_sp), tp) for j in range(1, n_sp)]
    peers += [(sp, lax.rem(tp + j, n_tp)) for j in range(1, n_tp)]
    for device in peers:
        pl.semaphore_signal(barrier, inc=1, device_id=device, device_id_type=MESH)
    inputs = [
        pltpu.make_async_copy(src, dst, in_sem.at[at])
        for at, (src, dst) in enumerate(
            (
                (routes_hbm, routes),
                (route_weights_hbm, route_weights),
                (docs_hbm, docs),
                (pool_in_hbm, pool_in),
                (pool_weight_hbm, pool_weight),
                (pool_gain_hbm, pool_gain),
                (norm_gain_hbm, norm_gain),
                (residual_hbm, residual),
            )
        )
    ]
    for copy in inputs:
        copy.start()
    for copy in inputs[2:6]:
        copy.wait()

    doc_row = docs[...].astype(jnp.float32)
    doc_column = jnp.broadcast_to(doc_row, (LANES, length)).T[:, 0:1]
    ext[0:LANES, :] = jnp.zeros((LANES, width), jnp.bfloat16)
    ext[LANES:, :] = pool_in[...]

    blocks = length // LANES
    away = (
        LANES
        + lax.broadcasted_iota(jnp.int32, (LANES, 2 * LANES), 0)
        - lax.broadcasted_iota(jnp.int32, (LANES, 2 * LANES), 1)
    )
    half = LANES // 2

    def pooled_spread(b):
        def block(owner, piece):
            if relay:
                return gathered.at[owner, pl.ds(b * LANES + piece * half, half), :]
            return gathered.at[owner, pl.ds(b * LANES, LANES), :]

        def several(count):
            return gathered.at[pl.ds(0, count), pl.ds(b * LANES, LANES), :]

        return Spread(n_tp, sp, tp, block, several, p_send.at[b], lambda group: p_recv.at[b, group])

    def pool(b, prior, begin=0, end=LANES):
        low = b * LANES
        near = (doc_column[low : low + LANES, :] == prior) & (away >= 0)
        groups = width // GD
        for g in range(groups):
            if groups % 4 == 0:
                span = 2 << (g % 4)
            else:
                span = lax.shift_left(jnp.int32(2), (tp * groups + g) % 4)
            weight = (near & (away < span)).astype(jnp.float32)
            at = slice(g * GD, (g + 1) * GD)
            count = jnp.sum(weight, axis=1, keepdims=True)
            total = jnp.dot(
                weight.astype(jnp.bfloat16), ext[low : low + 2 * LANES, at], preferred_element_type=jnp.float32
            )
            own = ext[low + LANES : low + 2 * LANES, at].astype(jnp.float32)
            diff = (total / count - own).astype(jnp.bfloat16)
            mixed = jnp.dot(diff, pool_weight[g], preferred_element_type=jnp.float32)
            pooled = (mixed * pool_gain[:, at]).astype(jnp.bfloat16)
            gathered[tp, low + begin : low + end, at] = pooled[begin:end]

    for b in range(1, blocks):
        pool(b, doc_row[:, (b - 1) * LANES : (b + 1) * LANES])

    pl.semaphore_wait(barrier, len(peers))

    def halo_copies(to):
        return [
            remote(docs.at[:, length - LANES :], halo_docs, h_send.at[0], h_recv.at[0], (to, tp)),
            remote(pool_in.at[length - TAIL :, :], halo, h_send.at[1], h_recv.at[1], (to, tp)),
        ]

    @pl.when(sp < n_sp - 1)
    def _():
        for copy in halo_copies(sp + 1):
            copy.start()

    for b in range(1, blocks):
        pooled_spread(b).start()
    for copy in inputs[:2] + inputs[6:]:
        copy.wait()
    for copy in loads:
        copy.start()

    high = max(16, experts)
    route = [routes[k : k + 1, :] for k in range(TOPK)]
    expert = lax.broadcasted_iota(jnp.int32, (high, length), 0)
    used = sum((expert == route[k]).astype(jnp.float32) for k in range(TOPK))
    before = lax.broadcasted_iota(jnp.int32, (length, length), 0) < lax.broadcasted_iota(
        jnp.int32, (length, length), 1
    )
    taken = jnp.dot(
        used.astype(jnp.bfloat16), before.astype(jnp.bfloat16), preferred_element_type=jnp.float32
    )
    slot = []
    for k in range(TOPK):
        rank = jnp.sum(jnp.where(expert == route[k], taken, 0.0), axis=0, keepdims=True)
        slot.append(route[k].astype(jnp.float32) * cap + rank)
    line = lax.broadcasted_iota(jnp.int32, (LANES, length), 0)
    table = jnp.zeros((LANES, length), jnp.float32)
    for k in range(TOPK):
        table = jnp.where(line == k, slot[k], table)
    columns = table.T
    slot_column = [columns[:, k : 1 + k] for k in range(TOPK)]

    none = jnp.full((1, LANES), -1.0, jnp.float32)
    if relay:
        pool(0, jnp.concatenate([none, doc_row[:, :LANES]], axis=1), half, LANES)
        for copy in pooled_spread(0).direct()[1:3]:
            copy.start()

    @pl.when(sp == 0)
    def _():
        halo[...] = jnp.zeros_like(halo)
        halo_docs[...] = jnp.full_like(halo_docs, -1)

    @pl.when(sp > 0)
    def _():
        for copy in halo_copies(sp - 1):
            copy.wait_recv()

    ext[LANES - TAIL : LANES, :] = halo[...]
    first_docs = halo_docs[...].astype(jnp.float32)
    pool(0, jnp.concatenate([first_docs, doc_row[:, :LANES]], axis=1), 0, half if relay else LANES)
    for copy in pooled_spread(0).direct()[0 :: 3 if relay else 1]:
        copy.start()

    def part(owner):
        deep = pl.ds(pl.multiple_of(owner * width, width), width)
        return jnp.dot(gathered[owner], wout[deep, :], preferred_element_type=jnp.float32)

    loads[0].wait()
    acc[...] = residual[...].astype(jnp.float32) + part(tp)
    late_first = list(range(1, blocks)) + [0]
    for b in late_first:
        pooled_spread(b).pass_on()
    if relay:
        for b in late_first:
            pooled_spread(b).finish_near()
        acc[...] += part(2 * (tp // 2) + 1 - tp % 2)
        acc[...] += part((tp + 2) % 4)
        for b in late_first:
            pooled_spread(b).finish()
        acc[...] += part(3 - tp)
    else:
        for b in late_first:
            pooled_spread(b).finish()

        @pl.loop(1, n_tp)
        def _(j):
            acc[...] += part(lax.rem(tp + j, n_tp))

    upf = acc[...].astype(jnp.bfloat16).astype(jnp.float32)
    acc[...] = upf
    gain = norm_gain[:, pl.ds(pl.multiple_of(tp * cols, LANES), cols)]
    plain = (acc[...] * gain).astype(jnp.bfloat16)

    def source(k):
        bits = range(max(1, (chips - 1).bit_length()))
        return sum(((my_chip // 2**b + k // 2**b) % 2) * 2**b for b in bits)

    inner = ((my_chip + 1) // 2) % 2

    def pick_by(i, mid, edge):
        value = 0
        for at, (a, b) in enumerate(zip(mid, edge)):
            value = value + jnp.where(i == at, b + (a - b) * inner, 0)
        return value

    held = chips == 4

    def group(k):
        return 0 if k == 0 else 2 if held and k == 2 else 1

    def dispatch(k, core):
        return remote(
            send.at[source(k), core],
            rows.at[my_chip, tp, my_core],
            d_send.at[group(k)],
            d_recv.at[my_chip],
            (source(k) * CORES + core, tp),
        )

    def dispatch_scale(k, core):
        return remote(
            scale_send.at[source(k), core],
            scale_rows.at[my_chip, my_core],
            e_send.at[group(k)],
            e_recv.at[my_chip],
            (source(k) * CORES + core, tp),
        )

    partner = (my_chip * CORES + 1 - my_core, tp)

    def dispatched(at):
        few = [1, 2] if held else [1, chips - 1]
        for buf, sem in ((send, d_send), (scale_send, e_send)):
            ref = buf.at[0, 0] if at == 0 else buf.at[0] if at == 2 else buf.at[pl.ds(0, few[1])]
            remote(ref, ref, sem.at[at], d_recv.at[0], partner).wait_send()

    def arrived(chip, sem, both, one):
        @pl.when(chip != my_chip)
        def _():
            remote(both, both, sem.at[chip], sem.at[chip], partner).wait_recv()

        @pl.when(chip == my_chip)
        def _():
            remote(one, one, sem.at[chip], sem.at[chip], partner).wait_recv()

    place = lax.broadcasted_iota(jnp.int32, (flat, length), 0).astype(jnp.float32)

    def choose(k):
        chip = source(k)
        here = place + (chip * flat).astype(jnp.float32)
        pick = sum((here == slot[j]).astype(jnp.float32) for j in range(TOPK)).astype(jnp.bfloat16)
        chosen = jnp.dot(pick, plain, preferred_element_type=jnp.float32).astype(jnp.bfloat16)
        send[chip] = chosen.reshape(CORES, cap, cols)
        if k == 0:
            rows[my_chip, tp, my_core] = send[my_chip, my_core]
            dispatch(0, 1 - my_core).start()

    def start_send(k, cores):
        for core in cores:
            dispatch(k, core).start()

    def spread_of(buf, ssem, rsem, chip):
        def block(owner, piece):
            return buf.at[chip, owner, piece] if relay else buf.at[chip, owner]

        def several(count):
            return buf.at[chip, pl.ds(0, count)]

        return Spread(n_tp, sp, tp, block, several, ssem.at[chip], lambda group: rsem.at[chip, group])

    def row_spread(chip):
        return spread_of(rows, f_send, f_recv, chip)

    def act_spread(chip):
        return spread_of(act, a_send, a_recv, chip)

    def await_rows(chip):
        arrived(chip, d_recv, rows.at[chip, tp], rows.at[chip, tp, 0])

    def start_rows(chip):
        await_rows(chip)
        row_spread(chip).start()

    first, rest = send_order(chips)

    def send_first(k):
        choose(k)
        if k:
            start_send(k, range(CORES))

    if held:

        @pl.when(inner == 1)
        def _():
            send_first(3)

    def start_own(core):
        @pl.when(my_core == core)
        def _():
            if core == 1 and relay:
                await_rows(my_chip)
                for copy in row_spread(my_chip).direct()[0::3]:
                    copy.start()
            else:
                start_rows(my_chip)

    send_first(0)
    squares = jnp.sum(acc[...] * acc[...], axis=1, keepdims=True)
    own = jnp.broadcast_to(squares, (length, LANES)).T[0:8]
    mine[...] = own
    small = [
        remote(mine, sums.at[tp], s_send.at[0], s_recv.at[0], (sp, lax.rem(tp + j, n_tp)))
        for j in range(1, n_tp)
    ]
    for copy in small:
        copy.start()

    def all_sums():
        ref = sums.at[pl.ds(0, n_tp - 1)]
        return remote(ref, ref, s_send.at[0], s_recv.at[0], (sp, lax.rem(tp + 1, n_tp)))

    start_own(0)
    if relay:

        @pl.when(my_core == 1)
        def _():
            for copy in row_spread(my_chip).direct()[1:3]:
                copy.start()

    for k in first[1:]:
        send_first(k)
    start_own(1)

    all_sums().wait_recv()
    for j in range(1, n_tp):
        own = own + sums[lax.rem(tp + n_tp - j, n_tp)]
    scale = lax.rsqrt(own[0:1] / (cols * n_tp) + EPS)
    slots_here = lax.broadcasted_iota(jnp.int32, (room, length), 0).astype(jnp.float32)
    for k in first + rest:
        chip = source(k)
        for core in range(CORES):
            here = slots_here + (chip * flat + core * cap).astype(jnp.float32)
            mine_here = sum(jnp.where(here == slot[j], scale, 0.0) for j in range(TOPK))
            weigh = sum(
                jnp.where(here == slot[j], route_weights[j : j + 1, :], 0.0) for j in range(TOPK)
            )
            pair = jnp.where(
                lax.broadcasted_iota(jnp.int32, (room, LANES), 1) == 0,
                jnp.sum(mine_here, axis=1, keepdims=True),
                jnp.sum(weigh, axis=1, keepdims=True),
            )
            scale_send[chip, core] = pair.T[0:8]

            @pl.when(chip * CORES + core == sp)
            def _():
                scale_rows[my_chip, my_core] = scale_send[my_chip, my_core]

            @pl.when(chip * CORES + core != sp)
            def _():
                dispatch_scale(k, core).start()

    for k in rest:

        @pl.when((inner == 0) | (k != 3))
        def _():
            choose(k)

    def hold(chip):
        @pl.when(inner == 1)
        def _():
            dispatched(1)
            for k in (1, 2, 3):
                for core in range(CORES):
                    pl.semaphore_signal(
                        credit, inc=1, device_id=(source(k) * CORES + core, tp), device_id_type=MESH
                    )
            pl.semaphore_wait(credit, CORES)
            start_send(2, range(CORES))

        @pl.when(inner == 0)
        def _():
            pl.semaphore_wait(credit, 2 * CORES)
            for k in rest:
                start_send(k, range(CORES))

    def give_back(chip, core, at=slice(None)):
        return remote(
            prod.at[chip, core, :, at],
            ret.at[my_chip, my_core, :, at],
            r_send.at[chip],
            r_recv.at[my_chip],
            (chip * CORES + core, tp),
        )

    tile = min(hidden, 256)
    wide = min(cols, 256)

    def slot_numbers(chip, which):
        return jnp.concatenate(
            [
                jnp.broadcast_to(scale_rows[chip, core, which : which + 1], (LANES, room)).T[:cap, 0:1]
                for core in range(CORES)
            ],
            axis=0,
        )

    def activate(chip):
        arrived(chip, e_recv, scale_rows.at[chip], scale_rows.at[chip, 0])
        column = slot_numbers(chip, 0)

        @pl.loop(0, hidden // tile)
        def _(n):
            at = pl.ds(pl.multiple_of(n * tile, tile), tile)
            gate = jnp.zeros((flat, tile), jnp.float32)
            up = jnp.zeros((flat, tile), jnp.float32)
            for t in range(n_tp):
                block = rows[chip, t].reshape(flat, cols)
                deep = pl.ds(t * cols, cols)
                gate += jnp.dot(block, w_gate[deep, at], preferred_element_type=jnp.float32)
                up += jnp.dot(block, w_up[deep, at], preferred_element_type=jnp.float32)
            value = (jax.nn.silu(gate * column) * (up * column)).astype(jnp.bfloat16)
            act[chip, tp, :, :, at] = value.reshape(CORES, cap, tile)

    def products(chip, owners, at):
        total = jnp.zeros((flat, wide), jnp.float32)
        for t in owners:
            block = act[chip, t].reshape(flat, hidden)
            deep = pl.ds(pl.multiple_of(t * hidden, hidden), hidden)
            total += jnp.dot(block, w_down[deep, at], preferred_element_type=jnp.float32)
        return total

    if relay:
        near, far = [tp, 2 * (tp // 2) + 1 - tp % 2, (tp + 2) % 4], [3 - tp]
    else:
        near, far = [tp], [lax.rem(tp + j, n_tp) for j in range(1, n_tp)]

    def tiles(n):
        return pl.ds(pl.multiple_of(n * wide, wide), wide)

    def produce_near(chip):
        @pl.loop(0, cols // wide)
        def _(n):
            partial[:, tiles(n)] = products(chip, near, tiles(n))

    def produce(chip):
        weigh = slot_numbers(chip, 1)

        @pl.loop(0, cols // wide)
        def _(n):
            at = tiles(n)
            total = (partial[:, at] + products(chip, far, at)) * weigh
            prod[chip, :, :, at] = total.astype(jnp.bfloat16).reshape(CORES, cap, wide)
            for core in range(CORES):

                @pl.when(chip * CORES + core != sp)
                def _():
                    give_back(chip, core, at).start()

    def finish_rows(chip):
        row_spread(chip).finish_near()
        row_spread(chip).finish()
        activate(chip)

    def finish_act(chip):
        act_spread(chip).finish_near()
        produce_near(chip)
        act_spread(chip).finish()
        produce(chip)

        @pl.when(chip == my_chip)
        def _():
            ret[my_chip, my_core] = prod[my_chip, my_core]

    lane = lax.broadcasted_iota(jnp.int32, (length, flat), 1).astype(jnp.float32)

    def returned(chip):
        here = lane + (chip * flat).astype(jnp.float32)
        pick = sum((slot_column[j] == here).astype(jnp.float32) for j in range(TOPK)).astype(jnp.bfloat16)
        arrived(chip, r_recv, ret.at[chip], ret.at[chip, 0])
        return acc[...] + jnp.dot(pick, ret[chip].reshape(flat, cols), preferred_element_type=jnp.float32)

    def combine(chip):
        acc[...] = returned(chip)

    def combine_last(chip):
        out[...] = returned(chip).astype(jnp.bfloat16)

    def settle(_chip):
        @pl.when(sp < n_sp - 1)
        def _():
            for copy in halo_copies(sp + 1):
                copy.wait_send()

        all_sums().wait_send()
        for b in range(blocks):
            pooled_spread(b).sent()
        dispatched(0)
        if held:

            @pl.when(inner == 0)
            def _():
                dispatched(1)

            dispatched(2)
        else:
            dispatched(1)

        @pl.loop(0, chips)
        def _(chip):
            row_spread(chip).sent()

    stages = [
        start_rows,
        lambda chip: row_spread(chip).pass_on(),
        finish_rows,
        lambda chip: act_spread(chip).start(),
        lambda chip: act_spread(chip).pass_on(),
        finish_act,
        combine,
        hold,
        combine_last,
        settle,
    ]
    mid, edge = [
        [STAGES.index(name) * chips + k for name, k in steps] for steps in schedules(chips)
    ]
    for copy in loads[1:]:
        copy.wait()

    @pl.loop(0, len(mid))
    def _(i):
        code = pick_by(i, mid, edge)
        chip = source(code % chips)
        for at, stage in enumerate(stages):

            @pl.when(code // chips == at)
            def _():
                stage(chip)

    @pl.loop(0, chips)
    def _(chip):
        act_spread(chip).sent()

        @pl.when(chip != my_chip)
        def _():
            remote(prod.at[chip], prod.at[chip], r_send.at[chip], r_recv.at[0], partner).wait_send()

        @pl.when(chip == my_chip)
        def _():
            remote(prod.at[chip, 0], prod.at[chip, 0], r_send.at[chip], r_recv.at[0], partner).wait_send()


def shards(
    residual,
    pool_in,
    docs,
    pool_weight,
    pool_gain,
    out_weight,
    norm_gain,
    routes,
    route_weights,
    w_gate,
    w_up,
    w_down,
):
    length, width = pool_in.shape
    cols = residual.shape[1]
    hidden = w_gate.shape[2]
    n_sp, n_tp = lax.axis_size("sp"), lax.axis_size("tp")
    chips = n_sp // CORES
    cap = length * TOPK * 3 // (2 * n_sp)
    room = -(-cap // LANES) * LANES
    blocks = length // LANES
    groups = 3 if n_tp == 4 else 1
    dma = pltpu.SemaphoreType.DMA
    vmem = pl.BlockSpec(memory_space=pltpu.VMEM)
    hbm = pl.BlockSpec(memory_space=pl.ANY)
    half = jnp.bfloat16
    return pl.pallas_call(
        functools.partial(layer_kernel, n_sp, n_tp),
        out_shape=pltpu.VMEM((length, cols), half),
        in_specs=[hbm] * 12,
        out_specs=vmem,
        scratch_shapes=[
            pltpu.VMEM((length, cols), half),
            pltpu.VMEM((length, width), half),
            pltpu.VMEM((1, length), jnp.int32),
            pltpu.VMEM(pool_weight.shape, half),
            pltpu.VMEM((1, width), jnp.float32),
            pltpu.VMEM((1, *norm_gain.shape), jnp.float32),
            pltpu.VMEM((TOPK, length), jnp.int32),
            pltpu.VMEM((TOPK, length), jnp.float32),
            pltpu.VMEM((LANES + length, width), half),
            pltpu.VMEM((TAIL, width), half),
            pltpu.VMEM((1, LANES), jnp.int32),
            pltpu.VMEM((n_tp, length, width), half),
            pltpu.VMEM((length, cols), jnp.float32),
            pltpu.VMEM((8, length), jnp.float32),
            pltpu.VMEM((n_tp, 8, length), jnp.float32),
            pltpu.VMEM((chips, CORES, cap, cols), half),
            pltpu.VMEM((chips, n_tp, CORES, cap, cols), half),
            pltpu.VMEM((chips, n_tp, CORES, cap, hidden), half),
            pltpu.VMEM((chips, CORES, cap, cols), half),
            pltpu.VMEM((chips, CORES, cap, cols), half),
            pltpu.VMEM((chips, CORES, 8, room), jnp.float32),
            pltpu.VMEM((chips, CORES, 8, room), jnp.float32),
            pltpu.VMEM((CORES * cap, cols), jnp.float32),
            pltpu.VMEM(out_weight.shape, half),
            pltpu.VMEM(w_gate.shape[1:], half),
            pltpu.VMEM(w_up.shape[1:], half),
            pltpu.VMEM(w_down.shape[1:], half),
            dma((8,)),
            dma((4,)),
            dma((2,)),
            dma((2,)),
            dma((blocks,)),
            dma((blocks, groups)),
            dma((1,)),
            dma((1,)),
            dma((3,)),
            dma((chips,)),
            dma((chips,)),
            dma((chips, groups)),
            dma((chips,)),
            dma((chips, groups)),
            dma((chips,)),
            dma((chips,)),
            dma((3,)),
            dma((chips,)),
            pltpu.SemaphoreType.REGULAR,
        ],
        compiler_params=pltpu.CompilerParams(
            collective_id=0, has_side_effects=True, vmem_limit_bytes=VMEM_LIMIT
        ),
    )(
        residual,
        pool_in,
        docs.reshape(1, length),
        pool_weight,
        pool_gain.reshape(1, width),
        norm_gain.reshape(1, -1),
        routes.T,
        route_weights.T,
        out_weight,
        w_gate[0],
        w_up[0],
        w_down[0],
    )


def solution(mesh):
    placed = (
        P("sp", "tp"),
        P("sp", "tp"),
        P("sp"),
        P("tp", None, None),
        P("tp"),
        P(None, "tp"),
        P(),
        P("sp", None),
        P("sp", None),
        P("sp", None, "tp"),
        P("sp", None, "tp"),
        P("sp", None, "tp"),
    )
    return jax.shard_map(
        shards, mesh=mesh, in_specs=placed, out_specs=P("sp", "tp"), check_vma=False
    )
```

```python
import functools

import jax
import jax.numpy as jnp
from jax import lax
from jax.experimental import pallas as pl
from jax.experimental.pallas import tpu as pltpu
from jax.sharding import PartitionSpec as P

GD = 128
TOPK = 2
EPS = 1e-06
MESH = pl.DeviceIdType.MESH
CORES = 2
LANES = 128
TAIL = 16
VMEM_LIMIT = 62 * 1024 * 1024


def remote(src, dst, send_sem, recv_sem, device):
    return pltpu.make_async_remote_copy(
        src_ref=src,
        dst_ref=dst,
        send_sem=send_sem,
        recv_sem=recv_sem,
        device_id=device,
        device_id_type=MESH,
    )


class Spread:
    def __init__(self, n_tp, sp, tp, block, blocks, send_sem, recv_sem, apart=0):
        self.apart = apart
        self.n_tp, self.sp, self.tp = n_tp, sp, tp
        self.block, self.blocks, self.send_sem, self.recv_sem = block, blocks, send_sem, recv_sem
        self.relay = n_tp == 4
        self.across = 2 * (tp // 2) + 1 - tp % 2
        self.along = (tp + 2) % 4
        self.other = self.across if self.relay else lax.rem(tp + 1, n_tp)

    def copy(self, owner, piece, group, peer):
        ref = self.block(owner, piece)
        return remote(ref, ref, self.send_sem, self.recv_sem(group), (self.sp, peer))

    def direct(self):
        if self.relay:
            return [
                self.copy(self.tp, 0, 0, self.across),
                self.copy(self.tp, 1, self.apart, self.along),
                self.copy(self.tp, 1, 1, self.across),
                self.copy(self.tp, 0, 1, self.along),
            ]
        return [self.copy(self.tp, 0, 0, lax.rem(self.tp + j, self.n_tp)) for j in range(1, self.n_tp)]

    def start(self):
        for copy in self.direct():
            copy.start()

    def all_of(self, group, count):
        ref = self.blocks(count)
        return remote(ref, ref, self.send_sem, self.recv_sem(group), (self.sp, self.other))

    def pass_on(self):
        if self.relay:
            self.all_of(0, 1).wait_recv()
            self.copy(self.across, 0, 2, self.along).start()
            self.copy(self.along, 1, 2, self.across).start()

    def pass_piece(self, piece):
        owner, peer = (self.across, self.along) if piece == 0 else (self.along, self.across)
        self.copy(owner, piece, self.apart * piece, peer).wait_recv()
        self.copy(owner, piece, 2, peer).start()

    def finish_near(self):
        if self.relay:
            self.all_of(1, 1).wait_recv()

    def finish(self):
        if self.relay:
            self.all_of(2, 1).wait_recv()
        else:
            self.all_of(0, self.n_tp - 1).wait_recv()

    def sent(self):
        self.all_of(0, self.n_tp - 1).wait_send()


STAGES = ["D", "RD", "CD", "A", "RA", "CA", "C", "Z", "E", "W"]
MID = (
    "RD0 Z0 D3 RD3",
    "D1 CD3 A3 RA3",
    "D2 CD0 CA3 RD2",
    "RD1 CD2 A2 RA2",
    "CD1 A1 CA2 RA1",
    "A0 CA1 C3 RA0",
    "C1 W0 CA0 C0",
    "E2",
)
EDGE = (
    "RD0 Z0 D1 CD0",
    "RD1 D3 RD3 D2",
    "CD3 CD1 A3 RA3",
    "RD2 A1 CA3 CD2",
    "RA1 A2 CA1 RA2",
    "A0 CA2 RA0 C3",
    "W0 CA0 C2 C0",
    "E1",
)


def schedules(chips):
    if chips == 4:
        return [[(step[:-1], int(step[-1])) for step in " ".join(plan).split()] for plan in (MID, EDGE)]
    steps = [("RD", 0)]
    for k in range(1, chips):
        steps += [("D", k), ("RD", k), ("CD", k - 1), ("A", k - 1), ("RA", k - 1), ("CA", k - 1)]
    last = chips - 1
    steps += [("CD", last), ("A", last), ("RA", last), ("CA", last)]
    steps += [("C", k) for k in range(chips - 1)] + [("W", 0), ("E", last)]
    return steps, steps


def send_order(chips):
    return ([0, 1], [3, 2]) if chips == 4 else (list(range(chips)), [])


def layer_kernel(
    n_sp,
    n_tp,
    residual_hbm,
    pool_in_hbm,
    docs_hbm,
    pool_weight_hbm,
    pool_gain_hbm,
    norm_gain_hbm,
    routes_hbm,
    route_weights_hbm,
    wout_hbm,
    gate_hbm,
    up_hbm,
    down_hbm,
    out,
    residual,
    pool_in,
    docs,
    pool_weight,
    pool_gain,
    norm_gain,
    routes,
    route_weights,
    ext,
    halo,
    halo_docs,
    gathered,
    acc,
    mine,
    sums,
    send,
    rows,
    act,
    prod,
    ret,
    scale_send,
    scale_rows,
    partial,
    wout,
    w_gate,
    w_up,
    w_down,
    in_sem,
    load_sem,
    h_send,
    h_recv,
    p_send,
    p_recv,
    s_send,
    s_recv,
    d_send,
    d_recv,
    f_send,
    f_recv,
    a_send,
    a_recv,
    r_send,
    r_recv,
    e_send,
    e_recv,
    credit,
):
    sp, tp = lax.axis_index("sp"), lax.axis_index("tp")
    chips = n_sp // CORES
    my_chip, my_core = sp // CORES, sp % CORES
    length, width = pool_in.shape
    cols = residual.shape[1]
    cap = send.shape[2]
    hidden = act.shape[4]
    flat = CORES * cap
    experts = n_sp
    relay = n_tp == 4
    room = -(-cap // LANES) * LANES

    loads = [
        pltpu.make_async_copy(wout_hbm, wout, load_sem.at[0]),
        pltpu.make_async_copy(gate_hbm, w_gate, load_sem.at[1]),
        pltpu.make_async_copy(up_hbm, w_up, load_sem.at[2]),
        pltpu.make_async_copy(down_hbm, w_down, load_sem.at[3]),
    ]
    barrier = pltpu.get_barrier_semaphore()
    peers = [(lax.rem(sp + j, n_sp), tp) for j in range(1, n_sp)]
    peers += [(sp, lax.rem(tp + j, n_tp)) for j in range(1, n_tp)]
    for device in peers:
        pl.semaphore_signal(barrier, inc=1, device_id=device, device_id_type=MESH)
    inputs = [
        pltpu.make_async_copy(src, dst, in_sem.at[at])
        for at, (src, dst) in enumerate(
            (
                (routes_hbm, routes),
                (route_weights_hbm, route_weights),
                (docs_hbm, docs),
                (pool_in_hbm, pool_in),
                (pool_weight_hbm, pool_weight),
                (pool_gain_hbm, pool_gain),
                (norm_gain_hbm, norm_gain),
                (residual_hbm, residual),
            )
        )
    ]
    for copy in inputs:
        copy.start()
    for copy in inputs[2:6]:
        copy.wait()

    doc_row = docs[...].astype(jnp.float32)
    doc_column = jnp.broadcast_to(doc_row, (LANES, length)).T[:, 0:1]
    ext[0:LANES, :] = jnp.zeros((LANES, width), jnp.bfloat16)
    ext[LANES:, :] = pool_in[...]

    blocks = length // LANES
    away = (
        LANES
        + lax.broadcasted_iota(jnp.int32, (LANES, 2 * LANES), 0)
        - lax.broadcasted_iota(jnp.int32, (LANES, 2 * LANES), 1)
    )

    def pooled_spread(b):
        def block(owner, piece):
            if relay and piece == min(b, 1):
                return gathered.at[owner, pl.ds(b * LANES, TAIL), :]
            if relay:
                return gathered.at[owner, pl.ds(b * LANES + TAIL, LANES - TAIL), :]
            return gathered.at[owner, pl.ds(b * LANES, LANES), :]

        def several(count):
            return gathered.at[pl.ds(0, count), pl.ds(b * LANES, LANES), :]

        return Spread(n_tp, sp, tp, block, several, p_send.at[b], lambda group: p_recv.at[b, group], 3)

    def pool(b, prior, begin=0, end=LANES):
        low = b * LANES
        near = (doc_column[low + begin : low + end, :] == prior) & (away[begin:end] >= 0)
        groups = width // GD
        for g in range(groups):
            if groups % 4 == 0:
                span = 2 << (g % 4)
            else:
                span = lax.shift_left(jnp.int32(2), (tp * groups + g) % 4)
            weight = (near & (away[begin:end] < span)).astype(jnp.float32)
            at = slice(g * GD, (g + 1) * GD)
            count = jnp.sum(weight, axis=1, keepdims=True)
            total = jnp.dot(
                weight.astype(jnp.bfloat16), ext[low : low + 2 * LANES, at], preferred_element_type=jnp.float32
            )
            own = ext[low + LANES + begin : low + LANES + end, at].astype(jnp.float32)
            diff = (total / count - own).astype(jnp.bfloat16)
            mixed = jnp.dot(diff, pool_weight[g], preferred_element_type=jnp.float32)
            pooled = (mixed * pool_gain[:, at]).astype(jnp.bfloat16)
            gathered[tp, low + begin : low + end, at] = pooled

    for b in range(1, blocks):
        pool(b, doc_row[:, (b - 1) * LANES : (b + 1) * LANES])
    if relay:
        none = jnp.full((1, LANES), -1.0, jnp.float32)
        pool(0, jnp.concatenate([none, doc_row[:, :LANES]], axis=1), TAIL, LANES)

    pl.semaphore_wait(barrier, len(peers))

    def halo_copies(to):
        return [
            remote(docs.at[:, length - LANES :], halo_docs, h_send.at[0], h_recv.at[0], (to, tp)),
            remote(pool_in.at[length - TAIL :, :], halo, h_send.at[1], h_recv.at[1], (to, tp)),
        ]

    @pl.when(sp < n_sp - 1)
    def _():
        for copy in halo_copies(sp + 1):
            copy.start()

    later = range(1, blocks)
    if relay:
        for b in later:
            pooled_spread(b).direct()[1].start()
            pooled_spread(b).direct()[0].start()
        for copy in pooled_spread(0).direct()[1:3]:
            copy.start()
        for b in later:
            for copy in pooled_spread(b).direct()[2:4]:
                copy.start()
    else:
        for b in later:
            pooled_spread(b).start()
    for copy in inputs[:2] + inputs[6:]:
        copy.wait()
    for copy in loads:
        copy.start()

    high = max(16, experts)
    route = [routes[k : k + 1, :] for k in range(TOPK)]
    expert = lax.broadcasted_iota(jnp.int32, (high, length), 0)
    used = sum((expert == route[k]).astype(jnp.float32) for k in range(TOPK))
    before = lax.broadcasted_iota(jnp.int32, (length, length), 0) < lax.broadcasted_iota(
        jnp.int32, (length, length), 1
    )
    taken = jnp.dot(
        used.astype(jnp.bfloat16), before.astype(jnp.bfloat16), preferred_element_type=jnp.float32
    )
    slot = []
    for k in range(TOPK):
        rank = jnp.sum(jnp.where(expert == route[k], taken, 0.0), axis=0, keepdims=True)
        slot.append(route[k].astype(jnp.float32) * cap + rank)
    line = lax.broadcasted_iota(jnp.int32, (LANES, length), 0)
    table = jnp.zeros((LANES, length), jnp.float32)
    for k in range(TOPK):
        table = jnp.where(line == k, slot[k], table)
    columns = table.T
    slot_column = [columns[:, k : 1 + k] for k in range(TOPK)]

    @pl.when(sp == 0)
    def _():
        halo[...] = jnp.zeros_like(halo)
        halo_docs[...] = jnp.full_like(halo_docs, -1)

    @pl.when(sp > 0)
    def _():
        for copy in halo_copies(sp - 1):
            copy.wait_recv()

    ext[LANES - TAIL : LANES, :] = halo[...]
    first_docs = halo_docs[...].astype(jnp.float32)
    pool(0, jnp.concatenate([first_docs, doc_row[:, :LANES]], axis=1), 0, TAIL if relay else LANES)
    for copy in pooled_spread(0).direct()[0 :: 3 if relay else 1]:
        copy.start()

    def part(owner):
        deep = pl.ds(pl.multiple_of(owner * width, width), width)
        return jnp.dot(gathered[owner], wout[deep, :], preferred_element_type=jnp.float32)

    loads[0].wait()
    acc[...] = residual[...].astype(jnp.float32) + part(tp)
    late_first = list(range(1, blocks)) + [0]
    if relay:
        for b in later:
            pooled_spread(b).pass_piece(0)
        pooled_spread(0).pass_piece(1)
        for b in later:
            pooled_spread(b).pass_piece(1)
        pooled_spread(0).pass_piece(0)
        for b in late_first:
            pooled_spread(b).finish_near()
        acc[...] += part(2 * (tp // 2) + 1 - tp % 2)
        acc[...] += part((tp + 2) % 4)
        for b in late_first:
            pooled_spread(b).finish()
        acc[...] += part(3 - tp)
    else:
        for b in late_first:
            pooled_spread(b).finish()

        @pl.loop(1, n_tp)
        def _(j):
            acc[...] += part(lax.rem(tp + j, n_tp))

    upf = acc[...].astype(jnp.bfloat16).astype(jnp.float32)
    acc[...] = upf
    gain = norm_gain[:, pl.ds(pl.multiple_of(tp * cols, LANES), cols)]
    plain = (acc[...] * gain).astype(jnp.bfloat16)

    def source(k):
        bits = range(max(1, (chips - 1).bit_length()))
        return sum(((my_chip // 2**b + k // 2**b) % 2) * 2**b for b in bits)

    inner = ((my_chip + 1) // 2) % 2

    def pick_by(i, mid, edge):
        value = 0
        for at, (a, b) in enumerate(zip(mid, edge)):
            value = value + jnp.where(i == at, b + (a - b) * inner, 0)
        return value

    held = chips == 4

    def group(k):
        return 0 if k == 0 else 2 if held and k == 2 else 1

    def dispatch(k, core):
        return remote(
            send.at[source(k), core],
            rows.at[my_chip, tp, my_core],
            d_send.at[group(k)],
            d_recv.at[my_chip],
            (source(k) * CORES + core, tp),
        )

    def dispatch_scale(k, core):
        return remote(
            scale_send.at[source(k), core],
            scale_rows.at[my_chip, my_core],
            e_send.at[group(k)],
            e_recv.at[my_chip],
            (source(k) * CORES + core, tp),
        )

    partner = (my_chip * CORES + 1 - my_core, tp)

    def dispatched(at):
        few = [1, 2] if held else [1, chips - 1]
        for buf, sem in ((send, d_send), (scale_send, e_send)):
            ref = buf.at[0, 0] if at == 0 else buf.at[0] if at == 2 else buf.at[pl.ds(0, few[1])]
            remote(ref, ref, sem.at[at], d_recv.at[0], partner).wait_send()

    def arrived(chip, sem, both, one):
        @pl.when(chip != my_chip)
        def _():
            remote(both, both, sem.at[chip], sem.at[chip], partner).wait_recv()

        @pl.when(chip == my_chip)
        def _():
            remote(one, one, sem.at[chip], sem.at[chip], partner).wait_recv()

    place = lax.broadcasted_iota(jnp.int32, (flat, length), 0).astype(jnp.float32)

    def choose(k):
        chip = source(k)
        here = place + (chip * flat).astype(jnp.float32)
        pick = sum((here == slot[j]).astype(jnp.float32) for j in range(TOPK)).astype(jnp.bfloat16)
        chosen = jnp.dot(pick, plain, preferred_element_type=jnp.float32).astype(jnp.bfloat16)
        send[chip] = chosen.reshape(CORES, cap, cols)
        if k == 0:
            rows[my_chip, tp, my_core] = send[my_chip, my_core]
            dispatch(0, 1 - my_core).start()

    def start_send(k, cores):
        for core in cores:
            dispatch(k, core).start()

    def spread_of(buf, ssem, rsem, chip):
        def block(owner, piece):
            return buf.at[chip, owner, piece] if relay else buf.at[chip, owner]

        def several(count):
            return buf.at[chip, pl.ds(0, count)]

        return Spread(n_tp, sp, tp, block, several, ssem.at[chip], lambda group: rsem.at[chip, group])

    def row_spread(chip):
        return spread_of(rows, f_send, f_recv, chip)

    def act_spread(chip):
        return spread_of(act, a_send, a_recv, chip)

    def await_rows(chip):
        arrived(chip, d_recv, rows.at[chip, tp], rows.at[chip, tp, 0])

    def start_rows(chip):
        await_rows(chip)
        row_spread(chip).start()

    first, rest = send_order(chips)

    def send_first(k):
        choose(k)
        if k:
            start_send(k, range(CORES))

    if held:

        @pl.when(inner == 1)
        def _():
            send_first(3)

    def start_own(core):
        @pl.when(my_core == core)
        def _():
            if core == 1 and relay:
                await_rows(my_chip)
                for copy in row_spread(my_chip).direct()[0::3]:
                    copy.start()
            else:
                start_rows(my_chip)

    send_first(0)
    squares = jnp.sum(acc[...] * acc[...], axis=1, keepdims=True)
    own = jnp.broadcast_to(squares, (length, LANES)).T[0:8]
    mine[...] = own
    small = [
        remote(mine, sums.at[tp], s_send.at[0], s_recv.at[0], (sp, lax.rem(tp + j, n_tp)))
        for j in range(1, n_tp)
    ]
    for copy in small:
        copy.start()

    def all_sums():
        ref = sums.at[pl.ds(0, n_tp - 1)]
        return remote(ref, ref, s_send.at[0], s_recv.at[0], (sp, lax.rem(tp + 1, n_tp)))

    start_own(0)
    if relay:

        @pl.when(my_core == 1)
        def _():
            for copy in row_spread(my_chip).direct()[1:3]:
                copy.start()

    for k in first[1:]:
        send_first(k)
    start_own(1)

    all_sums().wait_recv()
    for j in range(1, n_tp):
        own = own + sums[lax.rem(tp + n_tp - j, n_tp)]
    scale = lax.rsqrt(own[0:1] / (cols * n_tp) + EPS)
    slots_here = lax.broadcasted_iota(jnp.int32, (room, length), 0).astype(jnp.float32)
    for k in first + rest:
        chip = source(k)
        for core in range(CORES):
            here = slots_here + (chip * flat + core * cap).astype(jnp.float32)
            mine_here = sum(jnp.where(here == slot[j], scale, 0.0) for j in range(TOPK))
            weigh = sum(
                jnp.where(here == slot[j], route_weights[j : j + 1, :], 0.0) for j in range(TOPK)
            )
            pair = jnp.where(
                lax.broadcasted_iota(jnp.int32, (room, LANES), 1) == 0,
                jnp.sum(mine_here, axis=1, keepdims=True),
                jnp.sum(weigh, axis=1, keepdims=True),
            )
            scale_send[chip, core] = pair.T[0:8]

            @pl.when(chip * CORES + core == sp)
            def _():
                scale_rows[my_chip, my_core] = scale_send[my_chip, my_core]

            @pl.when(chip * CORES + core != sp)
            def _():
                dispatch_scale(k, core).start()

    for k in rest:

        @pl.when((inner == 0) | (k != 3))
        def _():
            choose(k)

    def hold(chip):
        @pl.when(inner == 1)
        def _():
            dispatched(1)
            for k in (1, 2, 3):
                for core in range(CORES):
                    pl.semaphore_signal(
                        credit, inc=1, device_id=(source(k) * CORES + core, tp), device_id_type=MESH
                    )
            pl.semaphore_wait(credit, CORES)
            start_send(2, range(CORES))

        @pl.when(inner == 0)
        def _():
            pl.semaphore_wait(credit, 2 * CORES)
            for k in rest:
                start_send(k, range(CORES))

    def give_back(chip, core, at=slice(None)):
        return remote(
            prod.at[chip, core, :, at],
            ret.at[my_chip, my_core, :, at],
            r_send.at[chip],
            r_recv.at[my_chip],
            (chip * CORES + core, tp),
        )

    tile = min(hidden, 256)
    wide = min(cols, 256)

    def slot_numbers(chip, which):
        return jnp.concatenate(
            [
                jnp.broadcast_to(scale_rows[chip, core, which : which + 1], (LANES, room)).T[:cap, 0:1]
                for core in range(CORES)
            ],
            axis=0,
        )

    def activate(chip):
        arrived(chip, e_recv, scale_rows.at[chip], scale_rows.at[chip, 0])
        column = slot_numbers(chip, 0)

        @pl.loop(0, hidden // tile)
        def _(n):
            at = pl.ds(pl.multiple_of(n * tile, tile), tile)
            gate = jnp.zeros((flat, tile), jnp.float32)
            up = jnp.zeros((flat, tile), jnp.float32)
            for t in range(n_tp):
                block = rows[chip, t].reshape(flat, cols)
                deep = pl.ds(t * cols, cols)
                gate += jnp.dot(block, w_gate[deep, at], preferred_element_type=jnp.float32)
                up += jnp.dot(block, w_up[deep, at], preferred_element_type=jnp.float32)
            value = (jax.nn.silu(gate * column) * (up * column)).astype(jnp.bfloat16)
            act[chip, tp, :, :, at] = value.reshape(CORES, cap, tile)

    def products(chip, owners, at):
        total = jnp.zeros((flat, wide), jnp.float32)
        for t in owners:
            block = act[chip, t].reshape(flat, hidden)
            deep = pl.ds(pl.multiple_of(t * hidden, hidden), hidden)
            total += jnp.dot(block, w_down[deep, at], preferred_element_type=jnp.float32)
        return total

    if relay:
        near, far = [tp, 2 * (tp // 2) + 1 - tp % 2, (tp + 2) % 4], [3 - tp]
    else:
        near, far = [tp], [lax.rem(tp + j, n_tp) for j in range(1, n_tp)]

    def tiles(n):
        return pl.ds(pl.multiple_of(n * wide, wide), wide)

    def produce_near(chip):
        @pl.loop(0, cols // wide)
        def _(n):
            partial[:, tiles(n)] = products(chip, near, tiles(n))

    def produce(chip):
        weigh = slot_numbers(chip, 1)

        @pl.loop(0, cols // wide)
        def _(n):
            at = tiles(n)
            total = (partial[:, at] + products(chip, far, at)) * weigh
            prod[chip, :, :, at] = total.astype(jnp.bfloat16).reshape(CORES, cap, wide)
            for core in range(CORES):

                @pl.when(chip * CORES + core != sp)
                def _():
                    give_back(chip, core, at).start()

    def finish_rows(chip):
        row_spread(chip).finish_near()
        row_spread(chip).finish()
        activate(chip)

    def finish_act(chip):
        act_spread(chip).finish_near()
        produce_near(chip)
        act_spread(chip).finish()
        produce(chip)

        @pl.when(chip == my_chip)
        def _():
            ret[my_chip, my_core] = prod[my_chip, my_core]

    lane = lax.broadcasted_iota(jnp.int32, (length, flat), 1).astype(jnp.float32)

    def returned(chip):
        here = lane + (chip * flat).astype(jnp.float32)
        pick = sum((slot_column[j] == here).astype(jnp.float32) for j in range(TOPK)).astype(jnp.bfloat16)
        arrived(chip, r_recv, ret.at[chip], ret.at[chip, 0])
        return acc[...] + jnp.dot(pick, ret[chip].reshape(flat, cols), preferred_element_type=jnp.float32)

    def combine(chip):
        acc[...] = returned(chip)

    def combine_last(chip):
        out[...] = returned(chip).astype(jnp.bfloat16)

    def settle(_chip):
        @pl.when(sp < n_sp - 1)
        def _():
            for copy in halo_copies(sp + 1):
                copy.wait_send()

        all_sums().wait_send()
        for b in range(blocks):
            pooled_spread(b).sent()
        dispatched(0)
        if held:

            @pl.when(inner == 0)
            def _():
                dispatched(1)

            dispatched(2)
        else:
            dispatched(1)

        @pl.loop(0, chips)
        def _(chip):
            row_spread(chip).sent()

    stages = [
        start_rows,
        lambda chip: row_spread(chip).pass_on(),
        finish_rows,
        lambda chip: act_spread(chip).start(),
        lambda chip: act_spread(chip).pass_on(),
        finish_act,
        combine,
        hold,
        combine_last,
        settle,
    ]
    mid, edge = [
        [STAGES.index(name) * chips + k for name, k in steps] for steps in schedules(chips)
    ]
    for copy in loads[1:]:
        copy.wait()

    @pl.loop(0, len(mid))
    def _(i):
        code = pick_by(i, mid, edge)
        chip = source(code % chips)
        for at, stage in enumerate(stages):

            @pl.when(code // chips == at)
            def _():
                stage(chip)

    @pl.loop(0, chips)
    def _(chip):
        act_spread(chip).sent()

        @pl.when(chip != my_chip)
        def _():
            remote(prod.at[chip], prod.at[chip], r_send.at[chip], r_recv.at[0], partner).wait_send()

        @pl.when(chip == my_chip)
        def _():
            remote(prod.at[chip, 0], prod.at[chip, 0], r_send.at[chip], r_recv.at[0], partner).wait_send()


def shards(
    residual,
    pool_in,
    docs,
    pool_weight,
    pool_gain,
    out_weight,
    norm_gain,
    routes,
    route_weights,
    w_gate,
    w_up,
    w_down,
):
    length, width = pool_in.shape
    cols = residual.shape[1]
    hidden = w_gate.shape[2]
    n_sp, n_tp = lax.axis_size("sp"), lax.axis_size("tp")
    chips = n_sp // CORES
    cap = length * TOPK * 3 // (2 * n_sp)
    room = -(-cap // LANES) * LANES
    blocks = length // LANES
    groups = 3 if n_tp == 4 else 1
    dma = pltpu.SemaphoreType.DMA
    vmem = pl.BlockSpec(memory_space=pltpu.VMEM)
    hbm = pl.BlockSpec(memory_space=pl.ANY)
    half = jnp.bfloat16
    return pl.pallas_call(
        functools.partial(layer_kernel, n_sp, n_tp),
        out_shape=pltpu.VMEM((length, cols), half),
        in_specs=[hbm] * 12,
        out_specs=vmem,
        scratch_shapes=[
            pltpu.VMEM((length, cols), half),
            pltpu.VMEM((length, width), half),
            pltpu.VMEM((1, length), jnp.int32),
            pltpu.VMEM(pool_weight.shape, half),
            pltpu.VMEM((1, width), jnp.float32),
            pltpu.VMEM((1, *norm_gain.shape), jnp.float32),
            pltpu.VMEM((TOPK, length), jnp.int32),
            pltpu.VMEM((TOPK, length), jnp.float32),
            pltpu.VMEM((LANES + length, width), half),
            pltpu.VMEM((TAIL, width), half),
            pltpu.VMEM((1, LANES), jnp.int32),
            pltpu.VMEM((n_tp, length, width), half),
            pltpu.VMEM((length, cols), jnp.float32),
            pltpu.VMEM((8, length), jnp.float32),
            pltpu.VMEM((n_tp, 8, length), jnp.float32),
            pltpu.VMEM((chips, CORES, cap, cols), half),
            pltpu.VMEM((chips, n_tp, CORES, cap, cols), half),
            pltpu.VMEM((chips, n_tp, CORES, cap, hidden), half),
            pltpu.VMEM((chips, CORES, cap, cols), half),
            pltpu.VMEM((chips, CORES, cap, cols), half),
            pltpu.VMEM((chips, CORES, 8, room), jnp.float32),
            pltpu.VMEM((chips, CORES, 8, room), jnp.float32),
            pltpu.VMEM((CORES * cap, cols), jnp.float32),
            pltpu.VMEM(out_weight.shape, half),
            pltpu.VMEM(w_gate.shape[1:], half),
            pltpu.VMEM(w_up.shape[1:], half),
            pltpu.VMEM(w_down.shape[1:], half),
            dma((8,)),
            dma((4,)),
            dma((2,)),
            dma((2,)),
            dma((blocks,)),
            dma((blocks, groups + 1)),
            dma((1,)),
            dma((1,)),
            dma((3,)),
            dma((chips,)),
            dma((chips,)),
            dma((chips, groups)),
            dma((chips,)),
            dma((chips, groups)),
            dma((chips,)),
            dma((chips,)),
            dma((3,)),
            dma((chips,)),
            pltpu.SemaphoreType.REGULAR,
        ],
        compiler_params=pltpu.CompilerParams(
            collective_id=0, has_side_effects=True, vmem_limit_bytes=VMEM_LIMIT
        ),
    )(
        residual,
        pool_in,
        docs.reshape(1, length),
        pool_weight,
        pool_gain.reshape(1, width),
        norm_gain.reshape(1, -1),
        routes.T,
        route_weights.T,
        out_weight,
        w_gate[0],
        w_up[0],
        w_down[0],
    )


def solution(mesh):
    placed = (
        P("sp", "tp"),
        P("sp", "tp"),
        P("sp"),
        P("tp", None, None),
        P("tp"),
        P(None, "tp"),
        P(),
        P("sp", None),
        P("sp", None),
        P("sp", None, "tp"),
        P("sp", None, "tp"),
        P("sp", None, "tp"),
    )
    return jax.shard_map(
        shards, mesh=mesh, in_specs=placed, out_specs=P("sp", "tp"), check_vma=False
    )
```
